32 devices in a mesh: grp: 2 (over y), sp: 4 (over z), tp: 4 (over x, core).
Axes of the slice: x: 2, y: 2, z: 4, core: 2. Of those that a mesh axis runs over, the one named last changes fastest.
Arguments:
- residual: bfloat16 [2048, 2048], P(('grp', 'sp')), parts along dimension 0, may hold values from -6 to 6
- queries: bfloat16 [2048, 1024], P(('grp', 'sp'), 'tp'), parts along dimension 0, may hold values from -400 to 400
- keys: bfloat16 [2048, 1024], P(('grp', 'sp'), 'tp'), parts along dimension 0, may hold values from -8 to 8
- values: bfloat16 [2048, 1024], P(('grp', 'sp'), 'tp'), parts along dimension 0, may hold values from -6 to 6
- log_gates: float32 [2048, 16], P(('grp', 'sp'), 'tp'), parts along dimension 0, may hold values from -126 to 0, as said below
- w_out: bfloat16 [1024, 2048], P('tp'), may hold values from -0.75 to 0.75
- norm_gain: float32 [2048], replicated, may hold values from 0.1 to 1.9
- w_gate: bfloat16 [2048, 5632], P('sp', 'tp'), may hold values from -0.125 to 0.125
- w_up: bfloat16 [2048, 5632], P('sp', 'tp'), may hold values from -0.125 to 0.125
- w_down: bfloat16 [5632, 2048], P('tp', 'sp'), may hold values from -0.078125 to 0.078125
Outputs:
- output: bfloat16 [2048, 2048], P(('grp', 'sp', 'tp')), parts along dimension 0
The draws below stay inside these ranges and needn't reach their ends.
There are 2 independent parts, one for each index of `grp`. The reference program is written for one: setup_inputs(seed, part) draws one part's arguments, and reference() takes and returns one part's arrays. A program takes and returns all parts, laid end to end along the dimension named above; an argument that names none is the same for every part. Nothing has to cross between parts.
Inputs may be any that keep to these rules, and one draw needn't show every extreme that they name: `log_gates`: never rises along positions.
All inputs are finite; a program needn't handle non-finite values.
Results may differ from the reference program's by a relative error of at most 0.014.
Values may be sent and summed in bfloat16 or wider, within the bound.
A program may use at most 128 MiB of HBM per device.

```python
import math
import jax
import jax.numpy as jnp
from jax import lax

D = 2048
ATTN_HEAD_COUNT = 16
HEAD_DIM = 64
FF = 5632
TOK_DEV = 256
SEQUENCE_TOKENS = 1024
N_TP = 4


def layout(key):
    random_seed_key = jax.random.fold_in(key, 31)
    random_ordering_key, random_shift_key, random_back_key, random_stride_key, random_spacing_key, random_strong_key, random_select_key, random_spike_key = jax.random.split(random_seed_key, 8)
    block_count = SEQUENCE_TOKENS // TOK_DEV
    inserted_count = block_count - 2
    quarter = max(TOK_DEV // 4, 1)
    head_order = jax.random.permutation(random_ordering_key, ATTN_HEAD_COUNT)
    gradual_heads = head_order < ATTN_HEAD_COUNT // 2
    block_ids = jnp.arange(inserted_count, dtype=jnp.int32) + 2
    places = block_ids * TOK_DEV + jax.random.randint(random_shift_key, (inserted_count,), 0, quarter)
    matches = (block_ids - 1) * TOK_DEV - 1 - jax.random.randint(random_back_key, (inserted_count,), 0, quarter)
    neighbours = matches - jax.random.randint(random_stride_key, (inserted_count,), 1, 5)
    score_gaps = jax.random.uniform(random_spacing_key, (inserted_count, ATTN_HEAD_COUNT), jnp.float32, 1.0, 2.5)
    strong_decline = jax.random.uniform(random_strong_key, (inserted_count, ATTN_HEAD_COUNT), jnp.float32, math.log(0.02), math.log(0.1))
    picked = jax.random.permutation(random_select_key, inserted_count)[:2]
    sudden_spike = jnp.any(jnp.arange(inserted_count, dtype=jnp.int32)[:, None] == picked[None, :], axis=1)
    sudden_decline = jax.random.uniform(random_spike_key, (inserted_count, ATTN_HEAD_COUNT), jnp.float32, math.log(0.5), math.log(0.8))
    gate_changes = jnp.where(gradual_heads[None, :], jnp.where(sudden_spike[:, None], sudden_decline, 0.0), strong_decline)
    return (gradual_heads, places, matches, neighbours, score_gaps, gate_changes)


def planted(key):
    gradual_heads, places, matches, neighbours, score_gaps, gate_changes = layout(key)
    key_query, key_keys = jax.random.split(jax.random.fold_in(key, 11), 2)
    row_width = ATTN_HEAD_COUNT * HEAD_DIM
    query_rows = jnp.clip(jax.random.normal(key_query, (SEQUENCE_TOKENS, row_width), jnp.float32), -6.0, 6.0)
    key_rows = jnp.clip(jax.random.normal(key_keys, (SEQUENCE_TOKENS, row_width), jnp.float32), -6.0, 6.0)
    inserted_count = places.shape[0]
    levels = jnp.array([8.0, 12.0, 16.0], jnp.float32)
    strength = levels[jnp.arange(inserted_count, dtype=jnp.int32) % 3][:, None, None]
    chosen = key_rows[matches].reshape(inserted_count, ATTN_HEAD_COUNT, HEAD_DIM)
    energy = jnp.maximum(jnp.sum(chosen * chosen, axis=-1, keepdims=True), 0.5 * HEAD_DIM)
    planted_rows = strength * 8.0 * math.sqrt(HEAD_DIM) * chosen / energy
    compensate = (score_gaps + gate_changes)[:, :, None]
    neighbour = chosen * (1.0 - compensate / (8.0 * strength))
    query_rows = jnp.clip(query_rows.at[places].set(planted_rows.reshape(inserted_count, row_width)), -400.0, 400.0)
    key_rows = key_rows.at[neighbours].set(neighbour.reshape(inserted_count, row_width))
    return (query_rows, key_rows)


def draw_queries(key, part):
    return planted(key)[0].astype(jnp.bfloat16)


def draw_keys(key, part):
    return planted(key)[1].astype(jnp.bfloat16)


def draw_log_gates(key, part):
    gradual_heads, places, matches, neighbours, score_gaps, gate_changes = layout(key)
    key_factor, key_jitter = jax.random.split(jax.random.fold_in(key, 23), 2)
    block_count = SEQUENCE_TOKENS // TOK_DEV
    block_factor = jnp.exp(jax.random.uniform(key_factor, (block_count, ATTN_HEAD_COUNT), jnp.float32, math.log(0.5), math.log(2.0)))
    block_factor = jnp.repeat(block_factor, TOK_DEV, axis=0)
    roughness = jax.random.uniform(key_jitter, (SEQUENCE_TOKENS, ATTN_HEAD_COUNT), jnp.float32, 0.5, 1.5)
    head_rates = jnp.where(gradual_heads, 0.5 / SEQUENCE_TOKENS, 1.0 / 40.0)
    forget_logits = -head_rates[None, :] * block_factor * roughness
    clusters = jnp.zeros((SEQUENCE_TOKENS, ATTN_HEAD_COUNT), jnp.float32).at[matches].set(gate_changes)
    return jnp.cumsum(forget_logits + clusters, axis=0)


def shard_levels(key, dims, cuts, least, largest):
    def one(position, shards_of):
        steps = jax.random.uniform(jax.random.fold_in(jax.random.fold_in(key, 6), position), (shards_of,), jnp.float32, least / len(cuts), largest / len(cuts))
        return jnp.repeat(jnp.exp(steps), dims[position] // shards_of).reshape((-1,) + (1,) * (len(dims) - position - 1))

    level = one(*cuts[0])
    for cut in cuts[1:]:
        level = level * one(*cut)
    return level


def gaussian(key, shape, spread, limit, shards=(), kind=jnp.bfloat16):
    loudness = shard_levels(key, shape, shards, -0.22, 0.18) if shards else 1.0
    entries = jax.random.normal(key, shape, jnp.float32) * spread * loudness
    return jnp.minimum(jnp.maximum(entries, -limit), limit).astype(kind)


def setup_inputs(seed: int = 0, part: int = 0) -> dict:
    seeds = jax.random.split(jax.random.key(seed), 11)
    part_splits = jax.random.split(jax.random.fold_in(seeds[10], part), 11)
    return {
        "residual": gaussian(part_splits[0], (SEQUENCE_TOKENS, D), 1.0, 6.0, ((0, 4),)),
        "queries": draw_queries(jax.random.fold_in(jax.random.fold_in(seeds[10], part), 71), part),
        "keys": draw_keys(jax.random.fold_in(jax.random.fold_in(seeds[10], part), 71), part),
        "values": gaussian(part_splits[3], (SEQUENCE_TOKENS, ATTN_HEAD_COUNT * HEAD_DIM), 1.0, 6.0, ((0, 4), (1, 4))),
        "log_gates": draw_log_gates(jax.random.fold_in(jax.random.fold_in(seeds[10], part), 71), part),
        "w_out": gaussian(seeds[5], (ATTN_HEAD_COUNT * HEAD_DIM, D), HEAD_DIM ** -0.5, 0.75, ((0, 4),)),
        "norm_gain": jnp.clip(1.0 + 0.18 * jax.random.normal(seeds[6], (D,), jnp.float32), 0.1, 1.9),
        "w_gate": gaussian(seeds[7], (D, FF), D ** -0.5, 0.125, ((0, 4), (1, 4))),
        "w_up": gaussian(seeds[8], (D, FF), D ** -0.5, 0.125, ((0, 4), (1, 4))),
        "w_down": gaussian(seeds[9], (FF, D), FF ** -0.5, 0.078125, ((0, 4), (1, 4))),
    }


def normalize(rows_in, gain):
    floats = rows_in.astype(jnp.float32)
    scaled = floats * lax.rsqrt(lax.optimization_barrier(jnp.mean(floats * floats, axis=-1, keepdims=True)) + 1e-06)
    return (scaled * gain).astype(jnp.bfloat16)

def group_sum(left, right, groups):
    rows_total = left.shape[0]
    width = left.shape[1] // groups
    left_groups = left.reshape(rows_total, groups, width).astype(jnp.float32)
    right_groups = right.reshape(groups, width, right.shape[1]).astype(jnp.float32)
    partial_terms = jnp.einsum('tgc,gcd->gtd', left_groups, right_groups).astype(jnp.bfloat16)
    partial_terms = lax.optimization_barrier(partial_terms)
    return lax.optimization_barrier(jnp.sum(partial_terms.astype(jnp.float32), axis=0))

def reference(residual, queries, keys, values, log_gates, w_out, norm_gain, w_gate, w_up, w_down):
    score_scale = HEAD_DIM ** (-0.5)
    query_heads = queries.reshape(SEQUENCE_TOKENS, ATTN_HEAD_COUNT, HEAD_DIM)
    key_heads = keys.reshape(SEQUENCE_TOKENS, ATTN_HEAD_COUNT, HEAD_DIM).astype(jnp.float32)
    value_heads = values.reshape(SEQUENCE_TOKENS, ATTN_HEAD_COUNT, HEAD_DIM).astype(jnp.float32)
    block_rows = math.gcd(SEQUENCE_TOKENS, 512)
    key_positions = jnp.arange(SEQUENCE_TOKENS, dtype=jnp.int32)

    def one_block(index_block):
        anchor = (index_block * block_rows).astype(jnp.int32)
        query_block = lax.dynamic_slice_in_dim(query_heads, anchor, block_rows, 0).astype(jnp.float32)
        gate_block = lax.dynamic_slice_in_dim(log_gates, anchor, block_rows, 0)
        scores = jnp.einsum('qhd,khd->hqk', query_block, key_heads) * score_scale
        scores = scores + gate_block.T[:, :, None] - log_gates.T[:, None, :]
        query_positions = anchor + jnp.arange(block_rows, dtype=jnp.int32)
        causal = query_positions[:, None] >= key_positions[None, :]
        scores = jnp.where(causal[None], scores, -jnp.inf)
        row_max = lax.optimization_barrier(jnp.max(scores, axis=-1, keepdims=True))
        weights = jnp.where(causal[None], jnp.exp(scores - row_max), 0.0)
        totals = lax.optimization_barrier(jnp.sum(weights, axis=-1))
        rounded = lax.optimization_barrier(weights.astype(jnp.bfloat16)).astype(jnp.float32)
        summed = jnp.einsum('hqk,khd->hqd', rounded, value_heads) / totals[:, :, None]
        return summed.transpose(1, 0, 2).reshape(block_rows, ATTN_HEAD_COUNT * HEAD_DIM).astype(jnp.bfloat16)
    attended = lax.map(one_block, jnp.arange(SEQUENCE_TOKENS // block_rows, dtype=jnp.int32))
    attended = attended.reshape(SEQUENCE_TOKENS, ATTN_HEAD_COUNT * HEAD_DIM)
    projected = group_sum(attended, w_out, N_TP)
    mixed = (residual.astype(jnp.float32) + projected).astype(jnp.bfloat16)
    normed = normalize(mixed, norm_gain)
    gate_proj = jnp.dot(normed, w_gate, preferred_element_type=jnp.float32)
    up_proj = jnp.dot(normed, w_up, preferred_element_type=jnp.float32)
    hidden = (jax.nn.silu(gate_proj) * up_proj).astype(jnp.bfloat16)
    down_sum = group_sum(hidden, w_down, N_TP)
    summed = mixed.astype(jnp.float32) + 0.5 * down_sum
    scaled = summed * lax.rsqrt(lax.optimization_barrier(jnp.mean(summed * summed, axis=-1, keepdims=True)) + 1e-06)
    return scaled.astype(jnp.bfloat16)
```

```python
import functools
import math

import jax
import jax.numpy as jnp
from jax import lax
from jax.experimental import pallas as pl
from jax.experimental.pallas import tpu as pltpu
from jax.sharding import PartitionSpec as P


def normalize(rows_in, gain):
    floats = rows_in.astype(jnp.float32)
    scaled = floats * lax.rsqrt(jnp.mean(floats * floats, axis=-1, keepdims=True) + 1e-06)
    return (scaled * gain).astype(jnp.bfloat16)


def attend(queries, keys, values, log_gates):
    row_count = queries.shape[0]
    head_count = log_gates.shape[1]
    head_width = queries.shape[1] // head_count
    score_scale = head_width ** (-0.5)
    first_row = lax.axis_index("sp") * row_count
    query_heads = queries.reshape(row_count, head_count, head_width)
    query_gates = log_gates.T
    query_positions = first_row + jnp.arange(row_count, dtype=jnp.int32)
    initial = (
        jnp.full((head_count, row_count), -1e30, jnp.float32),
        jnp.zeros((head_count, row_count), jnp.float32),
        jnp.zeros((head_count, row_count, head_width), jnp.float32),
    )
    carried = initial
    key_piece = lax.all_gather(keys.astype(jnp.float32), "sp", axis=0, tiled=True).astype(
        jnp.bfloat16
    )
    value_piece = lax.all_gather(values.astype(jnp.float32), "sp", axis=0, tiled=True).astype(
        jnp.bfloat16
    )
    gate_piece = lax.all_gather(log_gates, "sp", axis=0, tiled=True)
    length = key_piece.shape[0]
    block_rows = math.gcd(length, 2048)
    block_count = length // block_rows
    key_blocks = key_piece.reshape(block_count, block_rows, head_count, head_width)
    value_blocks = value_piece.reshape(block_count, block_rows, head_count, head_width)
    gate_blocks = gate_piece.reshape(block_count, block_rows, head_count)
    offsets = jnp.arange(block_count, dtype=jnp.int32) * block_rows

    def one_block(state, inputs):
        current_key_block, value_block, gate_block, offset = inputs

        def work(current):
            running_max, running_sum, accumulated = current
            scores = (
                jnp.einsum(
                    "qhd,khd->hqk",
                    query_heads,
                    current_key_block,
                    preferred_element_type=jnp.float32,
                )
                * score_scale
            )
            scores = scores + query_gates[:, :, None] - gate_block.T[:, None, :]
            key_positions = offset + jnp.arange(block_rows, dtype=jnp.int32)
            causal = (query_positions[:, None] >= key_positions[None, :])[None]
            scores = jnp.where(causal, scores, -1e30)
            new_max = jnp.maximum(running_max, jnp.max(scores, axis=-1))
            weights = jnp.where(causal, jnp.exp(scores - new_max[:, :, None]), 0.0)
            rescale = jnp.exp(running_max - new_max)
            running_sum = running_sum * rescale + jnp.sum(weights, axis=-1)
            product = jnp.einsum(
                "hqk,khd->hqd",
                weights.astype(jnp.bfloat16),
                value_block,
                preferred_element_type=jnp.float32,
            )
            accumulated = accumulated * rescale[:, :, None] + product
            return (new_max, running_sum, accumulated)

        state = lax.cond(offset <= first_row + row_count - 1, work, lambda current: current, state)
        return (state, None)

    carried, _ = lax.scan(one_block, carried, (key_blocks, value_blocks, gate_blocks, offsets))
    running_max, running_sum, accumulated = carried
    attended = accumulated / running_sum[:, :, None]
    return (
        attended.transpose(1, 0, 2).reshape(row_count, head_count * head_width).astype(jnp.bfloat16)
    )


def body(residual, queries, keys, values, log_gates, w_out, norm_gain, w_gate, w_up, w_down):
    attended = attend(queries, keys, values, log_gates)
    row_count = attended.shape[0]
    per_device = row_count // lax.axis_size("tp")
    my_first = lax.axis_index("tp") * per_device
    projected = lax.psum(
        jnp.dot(attended, w_out, preferred_element_type=jnp.float32).astype(jnp.bfloat16), "tp"
    ).astype(jnp.float32)
    mixed_all = (residual.astype(jnp.float32) + projected).astype(jnp.bfloat16)
    normed_all = normalize(mixed_all, norm_gain)
    mixed = lax.dynamic_slice_in_dim(mixed_all, my_first, per_device, 0)
    gate_whole = lax.all_gather(w_gate, "sp", axis=0, tiled=True)
    up_whole = lax.all_gather(w_up, "sp", axis=0, tiled=True)
    down_whole = lax.all_gather(w_down, "sp", axis=1, tiled=True)
    gate_proj = jnp.dot(normed_all, gate_whole, preferred_element_type=jnp.float32)
    up_proj = jnp.dot(normed_all, up_whole, preferred_element_type=jnp.float32)
    hidden = (jax.nn.silu(gate_proj) * up_proj).astype(jnp.bfloat16)
    down_sum = lax.psum_scatter(
        jnp.dot(hidden, down_whole, preferred_element_type=jnp.float32).astype(jnp.bfloat16),
        "tp",
        scatter_dimension=0,
        tiled=True,
    ).astype(jnp.float32)
    summed = mixed.astype(jnp.float32) + 0.5 * down_sum
    scaled = summed * lax.rsqrt(jnp.mean(summed * summed, axis=-1, keepdims=True) + 1e-06)
    return scaled.astype(jnp.bfloat16)


MESH = pl.DeviceIdType.MESH
PIECES = 2


def layer_kernel(
    n, tp, chunk,
    q_ref, k_ref, v_ref, gt_ref, residual_ref, w_out_ref, gain_ref, wg_ref, wu_ref, wd_ref,
    out_ref,
    k_all, v_all, gt_all, att, proj, pc_buf, px_send, px_buf, mixed, normed,
    wg_all, wu_all, wd_all, hid, part, c_buf, x_send, x_buf, z_send, z_buf, total_ref,
    kv_sems, w_sems, y_sems, pc_sems, px_sems, nz_sems, nx_sems, nc_sems, c_sems, x_sems, z_sems, o_sems,
):
    me = lax.axis_index("sp")
    t = lax.axis_index("tp")
    g = lax.axis_index("grp")
    x, c = t // 2, t % 2
    nx = tp // 2
    mate = x * 2 + (1 - c)
    rows = q_ref.shape[0]
    sub = rows // tp
    width = residual_ref.shape[1]
    heads = gt_ref.shape[0]
    head = q_ref.shape[1] // heads
    depth = wg_ref.shape[0]
    ff = wg_ref.shape[1]
    half = depth // 2
    dcols = wd_ref.shape[1]
    dhalf = dcols // 2
    GATE, UP, DOWN = range(3)

    def across(dx):
        return lax.rem(x + dx, nx)

    def per_me(work):
        for s in range(n):
            pl.when(me == s)(functools.partial(work, s))

    def remote(src, dst, send_sem, recv_sem, target):
        return pltpu.make_async_remote_copy(
            src_ref=src, dst_ref=dst, send_sem=send_sem, recv_sem=recv_sem,
            device_id=target, device_id_type=MESH,
        )

    def arrived(slot, sems, *index):
        remote(slot, slot, sems.at[(0, *index)], sems.at[(1, *index)], {"tp": mate}).wait_recv()

    barrier = pltpu.get_barrier_semaphore()
    for d in range(1, n):
        pl.semaphore_signal(barrier, inc=1, device_id={"sp": lax.rem(me + d, n)}, device_id_type=MESH)
    for dx in range(1, nx):
        pl.semaphore_signal(
            barrier, inc=1, device_id={"tp": across(dx) * 2 + c}, device_id_type=MESH
        )
    pl.semaphore_signal(barrier, inc=1, device_id={"tp": mate}, device_id_type=MESH)
    pl.semaphore_signal(barrier, inc=1, device_id={"grp": 1 - g}, device_id_type=MESH)
    pl.semaphore_wait(barrier, n - 1 + nx - 1 + 2)

    sent = [[] for _ in range(n)]

    def launch(s, make):
        make().start()
        sent[s].append(make)

    def kv_copy(s, o, i):
        own = (k_ref, v_ref, gt_ref)[i]
        held = (k_all, v_all, gt_all)[i].at[min(o, n - 2)]
        return remote(
            own if o == s else held, held, kv_sems.at[0, o, i], kv_sems.at[1, o, i], {"sp": s + 1}
        )

    def kv_send(s, o, i):
        launch(s, lambda: kv_copy(s, o, i))

    def kv_arrived(o, i):
        arrived((k_all, v_all, gt_all)[i].at[o], kv_sems, o, i)

    def size_of(j):
        return min(chunk, ff - j * chunk)

    def weight_slot(s, e, i, side):
        size = size_of(s)
        if i == DOWN:
            return wd_all.at[
                :size, pl.ds(pl.multiple_of(e * dcols + side * dhalf, 128), dhalf)
            ]
        held = (wg_all, wu_all)[i]
        return held.at[pl.ds(pl.multiple_of(e * depth + side * half, 16), half), :size]

    def weight_copy(s, j, i):
        place = pl.ds(j * chunk, size_of(j))
        if i == DOWN:
            src = wd_ref.at[place, pl.ds(pl.multiple_of(g * dhalf, 128), dhalf)]
        else:
            src = (wg_ref, wu_ref)[i].at[pl.ds(pl.multiple_of(g * half, 16), half), place]
        return remote(
            src, weight_slot(j, s, i, g), w_sems.at[0, j, i], w_sems.at[1, s, i], {"sp": j}
        )

    def weights(s, targets, pieces):
        for j in targets:
            for i in pieces:
                launch(s, lambda j=j, i=i: weight_copy(s, j, i))

    def relay_weights(s, e, pieces):
        for i in pieces:
            slot = weight_slot(s, e, i, g)
            arrived(slot, w_sems, e, i)

            def make(i=i):
                place = weight_slot(s, e, i, g)
                return remote(
                    place, place, y_sems.at[0, e, i], y_sems.at[1, e, i], {"grp": 1 - g}
                )

            launch(s, make)

    def weights_there(s, e, pieces):
        for i in pieces:
            arrived(weight_slot(s, e, i, 1 - g), y_sems, e, i)

    def own_copies(s):
        size = size_of(s)
        mine = pl.ds(s * chunk, size)
        return (
            pltpu.make_async_copy(
                wg_ref.at[:, mine], wg_all.at[pl.ds(s * depth, depth), :size], o_sems.at[0]
            ),
            pltpu.make_async_copy(
                wu_ref.at[:, mine], wu_all.at[pl.ds(s * depth, depth), :size], o_sems.at[1]
            ),
            pltpu.make_async_copy(
                wd_ref.at[mine, :], wd_all.at[:size, pl.ds(s * dcols, dcols)], o_sems.at[2]
            ),
        )

    def opening(s):
        if s < n - 1:
            for i in range(3):
                kv_send(s, s, i)
        weights(s, range(s - 1, -1, -1), (GATE, UP))
        if s == 0:
            weights(s, [1], (GATE, UP))
        for copy in own_copies(s):
            copy.start()
        size = size_of(s)
        if size < chunk:
            wg_all[:, size:] = jnp.zeros((n * depth, chunk - size), jnp.bfloat16)
            wu_all[:, size:] = jnp.zeros((n * depth, chunk - size), jnp.bfloat16)
            wd_all[size:, :] = jnp.zeros((chunk - size, n * dcols), jnp.bfloat16)
        for o in range(s, n - 1):
            k_all[o] = jnp.zeros_like(k_ref)
            v_all[o] = jnp.zeros_like(v_ref)
            gt_all[o] = jnp.zeros_like(gt_ref)
        for o in range(s - 1, -1, -1):
            for i in range(3):
                kv_arrived(o, i)
                if s < n - 1:
                    kv_send(s, o, i)
        if 0 < s < n - 1:
            weights(s, [s + 1], (GATE, UP))

    per_me(opening)

    pair = 128 // head
    lane = lax.broadcasted_iota(jnp.int32, (rows, 128), 1)
    causal = lax.broadcasted_iota(jnp.int32, (rows, rows), 0) >= lax.broadcasted_iota(
        jnp.int32, (rows, rows), 1
    )
    contract = (((1,), (1,)), ((), ()))
    filler = -heads % 8
    gates = gt_ref[...]
    if filler:
        gates = jnp.concatenate([gates, jnp.zeros((filler, rows), jnp.float32)], axis=0)
    gates = gates.T
    for p in range(heads // pair):
        cols = slice(p * 128, (p + 1) * 128)
        q_pair = q_ref[:, cols]
        joined = jnp.zeros((rows, 128), jnp.float32)
        for i in range(pair):
            h = p * pair + i
            inside = (lane >= i * head) & (lane < (i + 1) * head)
            q_head = jnp.where(inside, q_pair, jnp.zeros_like(q_pair))
            g_query = gates[:, h : h + 1]
            scores = []
            for o in range(n):
                k_pair = k_ref[:, cols] if o == n - 1 else k_all[o, :, cols]
                g_key = gt_ref[h : h + 1, :] if o == n - 1 else gt_all[o, h : h + 1, :]
                score = (
                    lax.dot_general(q_head, k_pair, contract, preferred_element_type=jnp.float32)
                    * head ** (-0.5)
                    + g_query
                    - g_key
                )
                allowed = causal if o == n - 1 else (jnp.zeros((rows, rows), jnp.int32) + me) > o
                scores.append(jnp.where(allowed, score, -1e30))
            peak = functools.reduce(
                jnp.maximum, [jnp.max(score, axis=-1, keepdims=True) for score in scores]
            )
            total = jnp.zeros((rows, 1), jnp.float32)
            summed = jnp.zeros((rows, 128), jnp.float32)
            for o in range(n):
                v_pair = v_ref[:, cols] if o == n - 1 else v_all[o, :, cols]
                weight = jnp.exp(scores[o] - peak)
                total += jnp.sum(weight, axis=-1, keepdims=True)
                summed += jnp.dot(
                    weight.astype(jnp.bfloat16), v_pair, preferred_element_type=jnp.float32
                )
            joined = jnp.where(inside, summed / total, joined)
        att[:, cols] = joined.astype(jnp.bfloat16)

    for k in range(width // 512):
        cols = slice(k * 512, (k + 1) * 512)
        proj[:, cols] = jnp.dot(
            att[...], w_out_ref[:, cols], preferred_element_type=jnp.float32
        ).astype(jnp.bfloat16)

    def block(index):
        return pl.ds(pl.multiple_of(index * sub, sub), sub)

    pc = [
        remote(
            proj.at[block(across(dx) * 2 + 1 - c)], pc_buf.at[dx],
            pc_sems.at[0, dx], pc_sems.at[1, dx], {"tp": mate},
        )
        for dx in range(nx)
    ]
    for dx in (*range(1, nx), 0):
        pc[dx].start()
    px = [
        remote(
            px_send.at[dx], px_buf.at[dx], px_sems.at[0, dx], px_sems.at[1, dx],
            {"tp": across(dx) * 2 + c},
        )
        for dx in range(nx)
    ]
    for dx in range(1, nx):
        pc[dx].wait_recv()
        px_send[dx] = (
            proj[block(across(dx) * 2 + c), :].astype(jnp.float32) + pc_buf[dx].astype(jnp.float32)
        ).astype(jnp.bfloat16)
        px[dx].start()
    pc[0].wait_recv()
    acc = proj[block(t), :].astype(jnp.float32) + pc_buf[0].astype(jnp.float32)
    for dx in range(1, nx):
        px[dx].wait_recv()
        acc += px_buf[dx].astype(jnp.float32)
    mix = (residual_ref[block(t), :].astype(jnp.float32) + acc).astype(jnp.bfloat16)
    mixed[...] = mix
    floats = mix.astype(jnp.float32)
    scale = lax.rsqrt(jnp.mean(floats * floats, axis=-1, keepdims=True) + 1e-06)
    normed[me, t] = (floats * scale * gain_ref[...]).astype(jnp.bfloat16)

    span = width // PIECES

    def row_slot(o, owner, k):
        return normed.at[o, owner, :, k * span : (k + 1) * span]

    def pass_rows(s, o, k):
        for way, j in ((0, s + 1), (1, s - 1)):
            if 0 <= j < n and (o == s or (o < s) == (way == 0)):

                def make(way=way, j=j):
                    slot = row_slot(o, t, k)
                    return remote(
                        slot, slot, nz_sems.at[way, o, k], nz_sems.at[2, o, k], {"sp": j}
                    )

                launch(s, make)

    def spread_rows(s, o, k):
        def to_mate():
            slot = row_slot(o, t, k)
            return remote(slot, slot, nc_sems.at[0, o, 0, k], nc_sems.at[1, o, 0, k], {"tp": mate})

        for dx in range(1, nx):

            def over(dx=dx):
                slot = row_slot(o, t, k)
                return remote(
                    slot, slot, nx_sems.at[0, o, dx, k], nx_sems.at[1, o, dx, k],
                    {"tp": across(dx) * 2 + c},
                )

            launch(s, over)
        launch(s, to_mate)

    def rows_in(s, *origins):
        for o in origins:
            for k in range(PIECES):
                slot = row_slot(o, t, k)
                remote(
                    slot, slot, nz_sems.at[0, o, k], nz_sems.at[2, o, k], {"tp": mate}
                ).wait_recv()
                pass_rows(s, o, k)
                spread_rows(s, o, k)

    def hand_over(s, *origins):
        for o in origins:
            for k in range(PIECES):
                for dx in range(1, nx):
                    owner = lax.rem(x + nx - dx, nx) * 2 + c
                    arrived(row_slot(o, owner, k), nx_sems, o, dx, k)

                    def make(o=o, dx=dx, k=k):
                        slot = row_slot(o, lax.rem(x + nx - dx, nx) * 2 + c, k)
                        return remote(
                            slot, slot, nc_sems.at[0, o, dx, k], nc_sems.at[1, o, dx, k],
                            {"tp": mate},
                        )

                    launch(s, make)

    def rows_ready(o):
        for k in range(PIECES):
            for dx in range(nx):
                owner = lax.rem(x + nx - dx, nx) * 2 + 1 - c
                arrived(row_slot(o, owner, k), nc_sems, o, dx, k)

    def exchange(s):
        up, down = range(s + 1, n), range(s - 1, -1, -1)
        below, above = list(down), list(up)
        for k in range(PIECES):
            pass_rows(s, s, k)
            spread_rows(s, s, k)
        if s == 0:
            weights(s, range(2, n), (GATE, UP))
        if s == 0:
            weights(s, up, (DOWN,))
        if s == n - 1:
            weights(s, down, (DOWN,))
        if 0 < s < n - 1:
            if s == 1:
                weights(s, [0], (DOWN,))
            if s == n - 2:
                weights(s, [n - 1], (DOWN,))
        first, second = (below, above) if s >= n // 2 else (above, below)
        near = second + first if 0 < s < n - 1 else first
        if 0 < s < n - 1:
            relay_weights(s, first[0], (GATE, UP))
        hand_over(s, s)
        if s == 0 or s == n - 1:
            relay_weights(s, near[0], (GATE, UP))
            for k, o in enumerate(near):
                rows_in(s, o)
                if k:
                    relay_weights(s, o, (GATE, UP))
                    hand_over(s, near[k - 1])
            hand_over(s, near[-1])
        else:
            rows_in(s, *below)
            if s < n - 2:
                weights(s, range(s + 2, n), (GATE, UP))
                weights(s, range(s + 1, n), (DOWN,))
            hand_over(s, *below)
            rest = [e for e in below + above if e != first[0]]
            for e in rest[:1]:
                relay_weights(s, e, (GATE, UP))
            rows_in(s, *above)
            if s > 1:
                weights(s, down, (DOWN,))
            for e in rest[1:]:
                relay_weights(s, e, (GATE, UP))
            hand_over(s, *above)
        for e in near:
            weights_there(s, e, (GATE, UP))
        for o in range(n):
            rows_ready(o)
        for copy in own_copies(s):
            copy.wait()

    per_me(exchange)

    for j in range(n):
        piece = normed[j].reshape(rows, width)
        gate = jnp.dot(piece, wg_all[...], preferred_element_type=jnp.float32)
        up = jnp.dot(piece, wu_all[...], preferred_element_type=jnp.float32)
        hid[j] = (gate / (1.0 + jnp.exp(-gate)) * up).astype(jnp.bfloat16)

    def span_of(e):
        return slice(e * dcols, (e + 1) * dcols)

    def down_part(e):
        for j in range(n):
            product = jnp.dot(
                hid[j], wd_all[:, span_of(e)], preferred_element_type=jnp.float32
            ).astype(jnp.bfloat16)
            part[j, :, :, :, span_of(e)] = product.reshape(nx, 2, sub, dcols)

    def c_copy(j, e):
        return remote(
            part.at[j, :, 1 - c, :, span_of(e)], c_buf.at[j, :, :, span_of(e)],
            c_sems.at[0, j, e], c_sems.at[1, j, e], {"tp": mate},
        )

    def x_copy(j, dx, e):
        return remote(
            x_send.at[j, dx, :, span_of(e)], x_buf.at[j, dx, :, span_of(e)],
            x_sems.at[0, j, dx, e], x_sems.at[1, j, dx, e], {"tp": across(dx) * 2 + c},
        )

    turn = [lax.rem(me + 1 + k, n) for k in range(n)]

    def over_x(e):
        for j in turn:
            c_copy(j, e).start()
        for j in turn:
            c_copy(j, e).wait_recv()
            for dx in range(1, nx):
                x_send[j, dx, :, span_of(e)] = (
                    part[j, across(dx), c, :, span_of(e)].astype(jnp.float32)
                    + c_buf[j, across(dx), :, span_of(e)].astype(jnp.float32)
                ).astype(jnp.bfloat16)
                x_copy(j, dx, e).start()

    def local_sum(j, e):
        acc = part[j, x, c, :, span_of(e)].astype(jnp.float32) + c_buf[
            j, x, :, span_of(e)
        ].astype(jnp.float32)
        for dx in range(1, nx):
            x_copy(j, dx, e).wait_recv()
            acc += x_buf[j, dx, :, span_of(e)].astype(jnp.float32)
        return acc

    def z_in(slot, e):
        place = z_buf.at[slot, :, span_of(e)]
        remote(
            place, place, z_sems.at[0, slot, e], z_sems.at[1, slot, e], {"tp": mate}
        ).wait_recv()
        return z_buf[slot, :, span_of(e)].astype(jnp.float32)

    def over_z(s, e):
        ups = list(range(n - 1, s, -1))
        downs = list(range(s))
        order = ups + downs if s < n // 2 else downs + ups
        for j in order:
            acc = local_sum(j, e)
            to = s + 1 if j > s else s - 1
            behind = s - 1 if j > s else s + 1
            if 0 <= behind < n:
                acc += z_in(j, e)
            z_send[j, :, span_of(e)] = acc.astype(jnp.bfloat16)
            slot = n if to == j and j < s else j

            def make(j=j, slot=slot, to=to):
                return remote(
                    z_send.at[j, :, span_of(e)], z_buf.at[slot, :, span_of(e)],
                    z_sems.at[0, j, e], z_sems.at[1, slot, e], {"sp": to},
                )

            launch(s, make)

    def finish(s, e):
        acc = local_sum(s, e)
        if s > 0:
            acc += z_in(s, e)
        if s < n - 1:
            acc += z_in(n, e)
        total_ref[:, span_of(e)] = mixed[:, span_of(e)].astype(jnp.float32) + 0.5 * acc

    def down_arrived(s, *blocks):
        for e in blocks:
            if e != s:
                relay_weights(s, e, (DOWN,))
        for e in blocks:
            if e != s:
                weights_there(s, e, (DOWN,))

    middle = list(range(1, n - 1))
    ends = [0, n - 1] if n > 1 else [0]
    per_me(lambda s: down_arrived(s, *middle))
    for e in middle:
        down_part(e)
        over_x(e)
    per_me(lambda s: down_arrived(s, *ends))
    for e in ends:
        down_part(e)
        over_x(e)
    for e in middle + ends:
        per_me(lambda s, e=e: over_z(s, e))
        per_me(lambda s, e=e: finish(s, e))
    summed = total_ref[...]
    scale = lax.rsqrt(jnp.mean(summed * summed, axis=-1, keepdims=True) + 1e-06)
    out_ref[...] = (summed * scale).astype(jnp.bfloat16)

    for copy in pc:
        copy.wait_send()
    for dx in range(1, nx):
        px[dx].wait_send()
    for e in range(n):
        for j in range(n):
            c_copy(j, e).wait_send()
            for dx in range(1, nx):
                x_copy(j, dx, e).wait_send()

    def all_sent(s):
        for make in sent[s]:
            make().wait_send()

    per_me(all_sent)


def fused_body(residual, queries, keys, values, log_gates, w_out, norm_gain, w_gate, w_up, w_down):
    n, tp = lax.axis_size("sp"), lax.axis_size("tp")
    rows, width = residual.shape
    sub = rows // tp
    nx = tp // 2
    depth, ff = w_gate.shape
    dcols = w_down.shape[1]
    chunk = window(ff, n)
    gates_t = log_gates.T
    bf16, f32 = jnp.bfloat16, jnp.float32
    shapes = [
        ((n - 1, *keys.shape), bf16),
        ((n - 1, *values.shape), bf16),
        ((n - 1, *gates_t.shape), f32),
        (queries.shape, bf16),
        ((rows, width), bf16),
        ((nx, sub, width), bf16),
        ((nx, sub, width), bf16),
        ((nx, sub, width), bf16),
        ((sub, width), bf16),
        ((n, tp, sub, width), bf16),
        ((n * depth, chunk), bf16),
        ((n * depth, chunk), bf16),
        ((chunk, n * dcols), bf16),
        ((n, rows, chunk), bf16),
        ((n, nx, 2, sub, width), bf16),
        ((n, nx, sub, width), bf16),
        ((n, nx, sub, width), bf16),
        ((n, nx, sub, width), bf16),
        ((n, sub, width), bf16),
        ((n + 1, sub, width), bf16),
        ((sub, width), f32),
    ]
    sems = [
        (2, n, 3),
        (2, n, 3),
        (2, n, 3),
        (2, nx),
        (2, nx),
        (3, n, PIECES),
        (2, n, nx, PIECES),
        (2, n, nx, PIECES),
        (2, n, n),
        (2, n, nx, n),
        (2, n + 1, n),
        (3,),
    ]
    return pl.pallas_call(
        functools.partial(layer_kernel, n, tp, chunk),
        out_shape=jax.ShapeDtypeStruct((sub, width), bf16),
        in_specs=[pl.BlockSpec(memory_space=pltpu.VMEM)] * 7
        + [pl.BlockSpec(memory_space=pl.ANY)] * 3,
        out_specs=pl.BlockSpec(memory_space=pltpu.VMEM),
        scratch_shapes=[pltpu.VMEM(shape, dtype) for shape, dtype in shapes]
        + [pltpu.SemaphoreType.DMA(shape) for shape in sems],
        compiler_params=pltpu.CompilerParams(
            collective_id=0, has_side_effects=True, vmem_limit_bytes=60 * 1024 * 1024
        ),
    )(
        queries, keys, values, gates_t, residual, w_out, norm_gain[None, :],
        w_gate, w_up, w_down,
    )


def window(ff, n):
    return -(-ff // (n * 128)) * 128


def fits(mesh, shapes):
    residual, queries, gates, gate = shapes
    n, tp, grp = mesh.shape["sp"], mesh.shape["tp"], mesh.shape["grp"]
    ff = gate[1] // tp
    heads = gates[1] // tp
    head = queries[1] // gates[1]
    rows = residual[0] // (grp * n)
    return (
        grp == 2
        and 2 <= n <= 4
        and tp % 2 == 0
        and ff % 128 == 0
        and window(ff, n) * (n - 1) < ff
        and 128 % head == 0
        and (heads * head) % 128 == 0
        and rows % (16 * tp) == 0
        and rows * n * residual[1] <= 1 << 21
    )


def solution(mesh):
    in_specs = (
        P(("grp", "sp"), None),
        P(("grp", "sp"), "tp"),
        P(("grp", "sp"), "tp"),
        P(("grp", "sp"), "tp"),
        P(("grp", "sp"), "tp"),
        P("tp", None),
        P(),
        P("sp", "tp"),
        P("sp", "tp"),
        P("tp", "sp"),
    )
    out_specs = P(("grp", "sp", "tp"), None)

    def layer(*args):
        residual, queries, _, _, log_gates, _, _, w_gate, _, _ = args
        shapes = (residual.shape, queries.shape, log_gates.shape, w_gate.shape)
        chosen = fused_body if fits(mesh, shapes) else body
        return jax.shard_map(
            chosen, mesh=mesh, in_specs=in_specs, out_specs=out_specs, check_vma=False
        )(*args)

    return layer
```

```python
import functools
import math

import jax
import jax.numpy as jnp
from jax import lax
from jax.experimental import pallas as pl
from jax.experimental.pallas import tpu as pltpu
from jax.sharding import PartitionSpec as P


def normalize(rows_in, gain):
    floats = rows_in.astype(jnp.float32)
    scaled = floats * lax.rsqrt(jnp.mean(floats * floats, axis=-1, keepdims=True) + 1e-06)
    return (scaled * gain).astype(jnp.bfloat16)


def attend(queries, keys, values, log_gates):
    row_count = queries.shape[0]
    head_count = log_gates.shape[1]
    head_width = queries.shape[1] // head_count
    score_scale = head_width ** (-0.5)
    first_row = lax.axis_index("sp") * row_count
    query_heads = queries.reshape(row_count, head_count, head_width)
    query_gates = log_gates.T
    query_positions = first_row + jnp.arange(row_count, dtype=jnp.int32)
    initial = (
        jnp.full((head_count, row_count), -1e30, jnp.float32),
        jnp.zeros((head_count, row_count), jnp.float32),
        jnp.zeros((head_count, row_count, head_width), jnp.float32),
    )
    carried = initial
    key_piece = lax.all_gather(keys.astype(jnp.float32), "sp", axis=0, tiled=True).astype(
        jnp.bfloat16
    )
    value_piece = lax.all_gather(values.astype(jnp.float32), "sp", axis=0, tiled=True).astype(
        jnp.bfloat16
    )
    gate_piece = lax.all_gather(log_gates, "sp", axis=0, tiled=True)
    length = key_piece.shape[0]
    block_rows = math.gcd(length, 2048)
    block_count = length // block_rows
    key_blocks = key_piece.reshape(block_count, block_rows, head_count, head_width)
    value_blocks = value_piece.reshape(block_count, block_rows, head_count, head_width)
    gate_blocks = gate_piece.reshape(block_count, block_rows, head_count)
    offsets = jnp.arange(block_count, dtype=jnp.int32) * block_rows

    def one_block(state, inputs):
        current_key_block, value_block, gate_block, offset = inputs

        def work(current):
            running_max, running_sum, accumulated = current
            scores = (
                jnp.einsum(
                    "qhd,khd->hqk",
                    query_heads,
                    current_key_block,
                    preferred_element_type=jnp.float32,
                )
                * score_scale
            )
            scores = scores + query_gates[:, :, None] - gate_block.T[:, None, :]
            key_positions = offset + jnp.arange(block_rows, dtype=jnp.int32)
            causal = (query_positions[:, None] >= key_positions[None, :])[None]
            scores = jnp.where(causal, scores, -1e30)
            new_max = jnp.maximum(running_max, jnp.max(scores, axis=-1))
            weights = jnp.where(causal, jnp.exp(scores - new_max[:, :, None]), 0.0)
            rescale = jnp.exp(running_max - new_max)
            running_sum = running_sum * rescale + jnp.sum(weights, axis=-1)
            product = jnp.einsum(
                "hqk,khd->hqd",
                weights.astype(jnp.bfloat16),
                value_block,
                preferred_element_type=jnp.float32,
            )
            accumulated = accumulated * rescale[:, :, None] + product
            return (new_max, running_sum, accumulated)

        state = lax.cond(offset <= first_row + row_count - 1, work, lambda current: current, state)
        return (state, None)

    carried, _ = lax.scan(one_block, carried, (key_blocks, value_blocks, gate_blocks, offsets))
    running_max, running_sum, accumulated = carried
    attended = accumulated / running_sum[:, :, None]
    return (
        attended.transpose(1, 0, 2).reshape(row_count, head_count * head_width).astype(jnp.bfloat16)
    )


def body(residual, queries, keys, values, log_gates, w_out, norm_gain, w_gate, w_up, w_down):
    attended = attend(queries, keys, values, log_gates)
    row_count = attended.shape[0]
    per_device = row_count // lax.axis_size("tp")
    my_first = lax.axis_index("tp") * per_device
    projected = lax.psum(
        jnp.dot(attended, w_out, preferred_element_type=jnp.float32).astype(jnp.bfloat16), "tp"
    ).astype(jnp.float32)
    mixed_all = (residual.astype(jnp.float32) + projected).astype(jnp.bfloat16)
    normed_all = normalize(mixed_all, norm_gain)
    mixed = lax.dynamic_slice_in_dim(mixed_all, my_first, per_device, 0)
    gate_whole = lax.all_gather(w_gate, "sp", axis=0, tiled=True)
    up_whole = lax.all_gather(w_up, "sp", axis=0, tiled=True)
    down_whole = lax.all_gather(w_down, "sp", axis=1, tiled=True)
    gate_proj = jnp.dot(normed_all, gate_whole, preferred_element_type=jnp.float32)
    up_proj = jnp.dot(normed_all, up_whole, preferred_element_type=jnp.float32)
    hidden = (jax.nn.silu(gate_proj) * up_proj).astype(jnp.bfloat16)
    down_sum = lax.psum_scatter(
        jnp.dot(hidden, down_whole, preferred_element_type=jnp.float32).astype(jnp.bfloat16),
        "tp",
        scatter_dimension=0,
        tiled=True,
    ).astype(jnp.float32)
    summed = mixed.astype(jnp.float32) + 0.5 * down_sum
    scaled = summed * lax.rsqrt(jnp.mean(summed * summed, axis=-1, keepdims=True) + 1e-06)
    return scaled.astype(jnp.bfloat16)


MESH = pl.DeviceIdType.MESH
PIECES = 2
OPENING = (
    (("kv",), ("gu", 1), ("dn", 1), ("gu", 2, 3), ("prep",)),
    (("kv",), ("gu", 0), ("dn", 0), ("prep",), ("kv_in", 0), ("gu", 2, 3), ("fwd", 2)),
    (("kv",), ("gu", 1, 0), ("prep",), ("kv_in", 1), ("kv_in", 0), ("gu", 3), ("dn", 3), ("fwd", 3)),
    (("gu", 2), ("dn", 2), ("gu", 1, 0), ("prep",), ("kv_in", 2), ("kv_in", 1), ("kv_in", 0)),
)
EXCHANGE = (
    (
        ("own",), ("fwd", 1), ("hand", 0), ("fwd", 3), ("fwd", 2), ("fwd_dn", 1), ("in", 1),
        ("in", 2), ("hand", 1), ("in", 3), ("dn", 2, 3), ("hand", 2), ("hand", 3),
    ),
    (
        ("own",), ("fwd", 0), ("fwd", 3), ("hand", 1), ("fwd_dn", 0), ("in", 2), ("in", 0),
        ("dn", 2, 3), ("in", 3), ("hand", 2), ("hand", 0), ("hand", 3),
    ),
    (
        ("own",), ("fwd", 0), ("hand", 2), ("in", 3), ("dn", 1, 0), ("fwd_dn", 3), ("fwd", 1),
        ("in", 1), ("hand", 3), ("in", 0), ("hand", 1), ("hand", 0),
    ),
    (
        ("own",), ("fwd", 2), ("fwd", 0), ("hand", 3), ("fwd_dn", 2), ("in", 2), ("fwd", 1),
        ("in", 1), ("dn", 1, 0), ("hand", 2), ("in", 0), ("hand", 1), ("hand", 0),
    ),
)
ROW_ORDER = ((0, 1, 2, 3), (1, 2, 3, 0), (2, 1, 0, 3), (3, 2, 1, 0))
COLUMN_ORDER = ((0, 1, 2, 3), (1, 0, 2, 3), (2, 3, 1, 0), (3, 2, 1, 0))


def line_tasks(n):
    ready = {}

    def when(s, j, e):
        if (s, j, e) not in ready:
            own = COLUMN_ORDER[s].index(e) * n + (ROW_ORDER[s].index(j) - 1) % n
            if j == s:
                before = [(b, j, e) for b in (s - 1, s + 1) if 0 <= b < n]
            else:
                b = s - 1 if j > s else s + 1
                before = [(b, j, e)] if 0 <= b < n else []
            ready[s, j, e] = max([own] + [when(*task) + 2 for task in before])
        return ready[s, j, e]

    every = [(j, e) for j in range(n) for e in range(n)]
    return [sorted(every, key=lambda task: (task[0] == s, when(s, *task), task)) for s in range(n)]


def layer_kernel(
    n, tp, chunk,
    q_ref, k_ref, v_ref, gt_ref, residual_ref, w_out_ref, gain_ref, wg_ref, wu_ref, wd_ref,
    out_ref,
    k_all, v_all, gt_all, att, proj, pc_buf, px_send, px_buf, mixed, normed,
    wg_all, wu_all, wd_all, hid, part, c_buf, x_send, x_buf, z_send, z_buf, total_ref,
    kv_sems, w_sems, y_sems, pc_sems, px_sems, nz_sems, nx_sems, nc_sems, c_sems, x_sems, z_sems, o_sems,
):
    me = lax.axis_index("sp")
    t = lax.axis_index("tp")
    g = lax.axis_index("grp")
    x, c = t // 2, t % 2
    nx = tp // 2
    mate = x * 2 + (1 - c)
    rows = q_ref.shape[0]
    sub = rows // tp
    width = residual_ref.shape[1]
    heads = gt_ref.shape[0]
    head = q_ref.shape[1] // heads
    depth = wg_ref.shape[0]
    ff = wg_ref.shape[1]
    half = depth // 2
    dcols = wd_ref.shape[1]
    dhalf = dcols // 2
    GATE, UP, DOWN = range(3)

    def across(dx):
        return lax.rem(x + dx, nx)

    def per_me(work):
        for s in range(n):

            @pl.when(me == s)
            def _(s=s):
                work(s)

    def remote(src, dst, send_sem, recv_sem, target):
        return pltpu.make_async_remote_copy(
            src_ref=src, dst_ref=dst, send_sem=send_sem, recv_sem=recv_sem,
            device_id=target, device_id_type=MESH,
        )

    def arrived(slot, sems, *index):
        remote(slot, slot, sems.at[(0, *index)], sems.at[(1, *index)], {"tp": mate}).wait_recv()

    barrier = pltpu.get_barrier_semaphore()
    for d in range(1, n):
        pl.semaphore_signal(barrier, inc=1, device_id={"sp": lax.rem(me + d, n)}, device_id_type=MESH)
    for dx in range(1, nx):
        pl.semaphore_signal(
            barrier, inc=1, device_id={"tp": across(dx) * 2 + c}, device_id_type=MESH
        )
    pl.semaphore_signal(barrier, inc=1, device_id={"tp": mate}, device_id_type=MESH)
    pl.semaphore_signal(barrier, inc=1, device_id={"grp": 1 - g}, device_id_type=MESH)
    pl.semaphore_wait(barrier, n - 1 + nx - 1 + 2)

    sent = [[] for _ in range(n)]

    def launch(s, make):
        make().start()
        sent[s].append(make)

    def kv_copy(s, o, i):
        own = (k_ref, v_ref, gt_ref)[i]
        held = (k_all, v_all, gt_all)[i].at[min(o, n - 2)]
        return remote(
            own if o == s else held, held, kv_sems.at[0, o, i], kv_sems.at[1, o, i], {"sp": s + 1}
        )

    def kv_send(s, o, i):
        launch(s, lambda: kv_copy(s, o, i))

    def kv_arrived(o, i):
        arrived((k_all, v_all, gt_all)[i].at[o], kv_sems, o, i)

    def size_of(j):
        return min(chunk, ff - j * chunk)

    def weight_slot(s, e, i, side):
        size = size_of(s)
        if i == DOWN:
            return wd_all.at[
                :size, pl.ds(pl.multiple_of(e * dcols + side * dhalf, 128), dhalf)
            ]
        held = (wg_all, wu_all)[i]
        return held.at[pl.ds(pl.multiple_of(e * depth + side * half, 16), half), :size]

    def weight_copy(s, j, i):
        place = pl.ds(j * chunk, size_of(j))
        if i == DOWN:
            src = wd_ref.at[place, pl.ds(pl.multiple_of(g * dhalf, 128), dhalf)]
        else:
            src = (wg_ref, wu_ref)[i].at[pl.ds(pl.multiple_of(g * half, 16), half), place]
        return remote(
            src, weight_slot(j, s, i, g), w_sems.at[0, j, i], w_sems.at[1, s, i], {"sp": j}
        )

    def weights(s, targets, pieces):
        for j in targets:
            for i in pieces:
                launch(s, lambda j=j, i=i: weight_copy(s, j, i))

    def relay_weights(s, e, pieces):
        for i in pieces:
            slot = weight_slot(s, e, i, g)
            arrived(slot, w_sems, e, i)

            def make(i=i):
                place = weight_slot(s, e, i, g)
                return remote(
                    place, place, y_sems.at[0, e, i], y_sems.at[1, e, i], {"grp": 1 - g}
                )

            launch(s, make)

    def weights_there(s, e, pieces):
        for i in pieces:
            arrived(weight_slot(s, e, i, 1 - g), y_sems, e, i)

    def own_copies(s):
        size = size_of(s)
        mine = pl.ds(s * chunk, size)
        return (
            pltpu.make_async_copy(
                wg_ref.at[:, mine], wg_all.at[pl.ds(s * depth, depth), :size], o_sems.at[0]
            ),
            pltpu.make_async_copy(
                wu_ref.at[:, mine], wu_all.at[pl.ds(s * depth, depth), :size], o_sems.at[1]
            ),
            pltpu.make_async_copy(
                wd_ref.at[mine, :], wd_all.at[:size, pl.ds(s * dcols, dcols)], o_sems.at[2]
            ),
        )

    span = width // PIECES

    def row_slot(o, owner, k):
        return normed.at[o, owner, :, k * span : (k + 1) * span]

    def pass_rows(s, o, k):
        for way, j in ((0, s + 1), (1, s - 1)):
            if 0 <= j < n and (o == s or (o < s) == (way == 0)):

                def make(way=way, j=j):
                    slot = row_slot(o, t, k)
                    return remote(
                        slot, slot, nz_sems.at[way, o, k], nz_sems.at[2, o, k], {"sp": j}
                    )

                launch(s, make)

    def spread_rows(s, o, k):
        def to_mate():
            slot = row_slot(o, t, k)
            return remote(slot, slot, nc_sems.at[0, o, 0, k], nc_sems.at[1, o, 0, k], {"tp": mate})

        for dx in range(1, nx):

            def over(dx=dx):
                slot = row_slot(o, t, k)
                return remote(
                    slot, slot, nx_sems.at[0, o, dx, k], nx_sems.at[1, o, dx, k],
                    {"tp": across(dx) * 2 + c},
                )

            launch(s, over)
        launch(s, to_mate)

    def rows_in(s, *origins):
        for o in origins:
            for k in range(PIECES):
                slot = row_slot(o, t, k)
                remote(
                    slot, slot, nz_sems.at[0, o, k], nz_sems.at[2, o, k], {"tp": mate}
                ).wait_recv()
                pass_rows(s, o, k)
                spread_rows(s, o, k)

    def hand_over(s, *origins):
        for o in origins:
            for k in range(PIECES):
                for dx in range(1, nx):
                    owner = lax.rem(x + nx - dx, nx) * 2 + c
                    arrived(row_slot(o, owner, k), nx_sems, o, dx, k)

                    def make(o=o, dx=dx, k=k):
                        slot = row_slot(o, lax.rem(x + nx - dx, nx) * 2 + c, k)
                        return remote(
                            slot, slot, nc_sems.at[0, o, dx, k], nc_sems.at[1, o, dx, k],
                            {"tp": mate},
                        )

                    launch(s, make)

    def rows_ready(o):
        for k in range(PIECES):
            for dx in range(nx):
                owner = lax.rem(x + nx - dx, nx) * 2 + 1 - c
                arrived(row_slot(o, owner, k), nc_sems, o, dx, k)

    def kv_in(s, o):
        for i in range(3):
            kv_arrived(o, i)
            if s < n - 1:
                kv_send(s, o, i)

    def kv_out(s):
        if s < n - 1:
            for i in range(3):
                kv_send(s, s, i)

    def prepare(s):
        for copy in own_copies(s):
            copy.start()
        size = size_of(s)
        if size < chunk:
            wg_all[:, size:] = jnp.zeros((n * depth, chunk - size), jnp.bfloat16)
            wu_all[:, size:] = jnp.zeros((n * depth, chunk - size), jnp.bfloat16)
            wd_all[size:, :] = jnp.zeros((chunk - size, n * dcols), jnp.bfloat16)
        for o in range(s, n - 1):
            k_all[o] = jnp.zeros_like(k_ref)
            v_all[o] = jnp.zeros_like(v_ref)
            gt_all[o] = jnp.zeros_like(gt_ref)

    def own_rows(s):
        for k in range(PIECES):
            pass_rows(s, s, k)
            spread_rows(s, s, k)

    steps = {
        "kv": kv_out,
        "kv_in": kv_in,
        "own": own_rows,
        "gu": lambda s, *to: weights(s, to, (GATE, UP)),
        "dn": lambda s, *to: weights(s, to, (DOWN,)),
        "in": lambda s, *origins: rows_in(s, *origins),
        "hand": lambda s, *origins: hand_over(s, *origins),
        "fwd": lambda s, e: relay_weights(s, e, (GATE, UP)),
        "fwd_dn": lambda s, e: relay_weights(s, e, (DOWN,)),
        "prep": prepare,
    }

    def follow(s, plan):
        for name, *where in plan:
            steps[name](s, *where)

    per_me(lambda s: follow(s, OPENING[s]))

    pair = 128 // head
    lane = lax.broadcasted_iota(jnp.int32, (rows, 128), 1)
    causal = lax.broadcasted_iota(jnp.int32, (rows, rows), 0) >= lax.broadcasted_iota(
        jnp.int32, (rows, rows), 1
    )
    contract = (((1,), (1,)), ((), ()))
    filler = -heads % 8
    gates = gt_ref[...]
    if filler:
        gates = jnp.concatenate([gates, jnp.zeros((filler, rows), jnp.float32)], axis=0)
    gates = gates.T
    for p in range(heads // pair):
        cols = slice(p * 128, (p + 1) * 128)
        q_pair = q_ref[:, cols]
        joined = jnp.zeros((rows, 128), jnp.float32)
        for i in range(pair):
            h = p * pair + i
            inside = (lane >= i * head) & (lane < (i + 1) * head)
            q_head = jnp.where(inside, q_pair, jnp.zeros_like(q_pair))
            g_query = gates[:, h : h + 1]
            scores = []
            for o in range(n):
                k_pair = k_ref[:, cols] if o == n - 1 else k_all[o, :, cols]
                g_key = gt_ref[h : h + 1, :] if o == n - 1 else gt_all[o, h : h + 1, :]
                score = (
                    lax.dot_general(q_head, k_pair, contract, preferred_element_type=jnp.float32)
                    * head ** (-0.5)
                    + g_query
                    - g_key
                )
                allowed = causal if o == n - 1 else (jnp.zeros((rows, rows), jnp.int32) + me) > o
                scores.append(jnp.where(allowed, score, -1e30))
            peak = functools.reduce(
                jnp.maximum, [jnp.max(score, axis=-1, keepdims=True) for score in scores]
            )
            total = jnp.zeros((rows, 1), jnp.float32)
            summed = jnp.zeros((rows, 128), jnp.float32)
            for o in range(n):
                v_pair = v_ref[:, cols] if o == n - 1 else v_all[o, :, cols]
                weight = jnp.exp(scores[o] - peak)
                total += jnp.sum(weight, axis=-1, keepdims=True)
                summed += jnp.dot(
                    weight.astype(jnp.bfloat16), v_pair, preferred_element_type=jnp.float32
                )
            joined = jnp.where(inside, summed / total, joined)
        att[:, cols] = joined.astype(jnp.bfloat16)

    for k in range(width // 512):
        cols = slice(k * 512, (k + 1) * 512)
        proj[:, cols] = jnp.dot(
            att[...], w_out_ref[:, cols], preferred_element_type=jnp.float32
        ).astype(jnp.bfloat16)

    def block(index):
        return pl.ds(pl.multiple_of(index * sub, sub), sub)

    pc = [
        remote(
            proj.at[block(across(dx) * 2 + 1 - c)], pc_buf.at[dx],
            pc_sems.at[0, dx], pc_sems.at[1, dx], {"tp": mate},
        )
        for dx in range(nx)
    ]
    for dx in (*range(1, nx), 0):
        pc[dx].start()
    px = [
        remote(
            px_send.at[dx], px_buf.at[dx], px_sems.at[0, dx], px_sems.at[1, dx],
            {"tp": across(dx) * 2 + c},
        )
        for dx in range(nx)
    ]
    for dx in range(1, nx):
        pc[dx].wait_recv()
        px_send[dx] = (
            proj[block(across(dx) * 2 + c), :].astype(jnp.float32) + pc_buf[dx].astype(jnp.float32)
        ).astype(jnp.bfloat16)
        px[dx].start()
    pc[0].wait_recv()
    acc = proj[block(t), :].astype(jnp.float32) + pc_buf[0].astype(jnp.float32)
    for dx in range(1, nx):
        px[dx].wait_recv()
        acc += px_buf[dx].astype(jnp.float32)
    mix = (residual_ref[block(t), :].astype(jnp.float32) + acc).astype(jnp.bfloat16)
    mixed[...] = mix
    floats = mix.astype(jnp.float32)
    scale = lax.rsqrt(jnp.mean(floats * floats, axis=-1, keepdims=True) + 1e-06)
    normed[me, t] = (floats * scale * gain_ref[...]).astype(jnp.bfloat16)

    def exchange(s):
        follow(s, EXCHANGE[s])
        for e in range(n):
            if e != s:
                weights_there(s, e, (GATE, UP))
        for copy in own_copies(s):
            copy.wait()

    per_me(exchange)

    def span_of(e):
        return pl.ds(e * dcols if isinstance(e, int) else pl.multiple_of(e * dcols, 128), dcols)

    def c_copy(j, e):
        return remote(
            part.at[j, :, 1 - c, :, span_of(e)], c_buf.at[j, :, :, span_of(e)],
            c_sems.at[0, j, e], c_sems.at[1, j, e], {"tp": mate},
        )

    def x_copy(j, dx, e):
        return remote(
            x_send.at[j, dx, :, span_of(e)], x_buf.at[j, dx, :, span_of(e)],
            x_sems.at[0, j, dx, e], x_sems.at[1, j, dx, e], {"tp": across(dx) * 2 + c},
        )

    high = me // (n // 2)
    row_order = [lax.rem(me + n + k * (1 - 2 * high), n) for k in range(n)]
    column_order = [me, me + 1 - 2 * lax.rem(me, 2), n // 2 - high, (n - 1) * (1 - high)]

    def down_part(j, e):
        product = jnp.dot(
            hid[j], wd_all[:, span_of(e)], preferred_element_type=jnp.float32
        ).astype(jnp.bfloat16)
        part[j, :, :, :, span_of(e)] = product.reshape(nx, 2, sub, dcols)
        c_copy(j, e).start()

    def over_x(j, e):
        c_copy(j, e).wait_recv()
        for dx in range(1, nx):
            x_send[j, dx, :, span_of(e)] = (
                part[j, across(dx), c, :, span_of(e)].astype(jnp.float32)
                + c_buf[j, across(dx), :, span_of(e)].astype(jnp.float32)
            ).astype(jnp.bfloat16)
            x_copy(j, dx, e).start()

    for k, j in enumerate(row_order):
        per_me(lambda s: rows_ready(ROW_ORDER[s][k]))
        piece = normed[j].reshape(rows, width)
        gate = jnp.dot(piece, wg_all[...], preferred_element_type=jnp.float32)
        up = jnp.dot(piece, wu_all[...], preferred_element_type=jnp.float32)
        hid[j] = (gate / (1.0 + jnp.exp(-gate)) * up).astype(jnp.bfloat16)
        down_part(j, column_order[0])
        if k:
            over_x(row_order[k - 1], column_order[0])
    over_x(row_order[-1], column_order[0])

    def local_sum(j, e):
        acc = part[j, x, c, :, span_of(e)].astype(jnp.float32) + c_buf[
            j, x, :, span_of(e)
        ].astype(jnp.float32)
        for dx in range(1, nx):
            x_copy(j, dx, e).wait_recv()
            acc += x_buf[j, dx, :, span_of(e)].astype(jnp.float32)
        return acc

    def z_in(slot, e):
        place = z_buf.at[slot, :, span_of(e)]
        remote(
            place, place, z_sems.at[0, slot, e], z_sems.at[1, slot, e], {"tp": mate}
        ).wait_recv()
        return z_buf[slot, :, span_of(e)].astype(jnp.float32)

    def over_z(s, j, e):
        acc = local_sum(j, e)
        to = s + 1 if j > s else s - 1
        behind = s - 1 if j > s else s + 1
        if 0 <= behind < n:
            acc += z_in(j, e)
        z_send[j, :, span_of(e)] = acc.astype(jnp.bfloat16)
        slot = n if to == j and j < s else j

        def make():
            return remote(
                z_send.at[j, :, span_of(e)], z_buf.at[slot, :, span_of(e)],
                z_sems.at[0, j, e], z_sems.at[1, slot, e], {"sp": to},
            )

        launch(s, make)

    def finish(s, e):
        acc = local_sum(s, e)
        if s > 0:
            acc += z_in(s, e)
        if s < n - 1:
            acc += z_in(n, e)
        total_ref[:, span_of(e)] = mixed[:, span_of(e)].astype(jnp.float32) + 0.5 * acc

    def down_arrived(s, e):
        if (("fwd_dn", e)) not in EXCHANGE[s]:
            relay_weights(s, e, (DOWN,))

    def down_there(s, e):
        weights_there(s, e, (DOWN,))

    order = line_tasks(n)

    def early(s, j, e):
        return s in (0, n - 1) and e == s and j != s

    def along(s, first):
        for j, e in order[s]:
            if early(s, j, e) == first:
                if j == s:
                    finish(s, e)
                else:
                    over_z(s, j, e)

    for q in range(1, n):
        if q == 1:
            per_me(lambda s: [down_arrived(s, e) for e in COLUMN_ORDER[s][1:]])
        per_me(lambda s: down_there(s, COLUMN_ORDER[s][q]))
        for j in row_order:
            down_part(j, column_order[q])
        for j in row_order[1:] + row_order[:1]:
            over_x(j, column_order[q])
        if q == 1:
            per_me(lambda s: along(s, True))

    per_me(lambda s: along(s, False))
    summed = total_ref[...]
    scale = lax.rsqrt(jnp.mean(summed * summed, axis=-1, keepdims=True) + 1e-06)
    out_ref[...] = (summed * scale).astype(jnp.bfloat16)

    for copy in pc:
        copy.wait_send()
    for dx in range(1, nx):
        px[dx].wait_send()
    for e in range(n):
        for j in range(n):
            c_copy(j, e).wait_send()
            for dx in range(1, nx):
                x_copy(j, dx, e).wait_send()

    def all_sent(s):
        for make in sent[s]:
            make().wait_send()

    per_me(all_sent)


def fused_body(residual, queries, keys, values, log_gates, w_out, norm_gain, w_gate, w_up, w_down):
    n, tp = lax.axis_size("sp"), lax.axis_size("tp")
    rows, width = residual.shape
    sub = rows // tp
    nx = tp // 2
    depth, ff = w_gate.shape
    dcols = w_down.shape[1]
    chunk = window(ff, n)
    gates_t = log_gates.T
    bf16, f32 = jnp.bfloat16, jnp.float32
    shapes = [
        ((n - 1, *keys.shape), bf16),
        ((n - 1, *values.shape), bf16),
        ((n - 1, *gates_t.shape), f32),
        (queries.shape, bf16),
        ((rows, width), bf16),
        ((nx, sub, width), bf16),
        ((nx, sub, width), bf16),
        ((nx, sub, width), bf16),
        ((sub, width), bf16),
        ((n, tp, sub, width), bf16),
        ((n * depth, chunk), bf16),
        ((n * depth, chunk), bf16),
        ((chunk, n * dcols), bf16),
        ((n, rows, chunk), bf16),
        ((n, nx, 2, sub, width), bf16),
        ((n, nx, sub, width), bf16),
        ((n, nx, sub, width), bf16),
        ((n, nx, sub, width), bf16),
        ((n, sub, width), bf16),
        ((n + 1, sub, width), bf16),
        ((sub, width), f32),
    ]
    sems = [
        (2, n, 3),
        (2, n, 3),
        (2, n, 3),
        (2, nx),
        (2, nx),
        (3, n, PIECES),
        (2, n, nx, PIECES),
        (2, n, nx, PIECES),
        (2, n, n),
        (2, n, nx, n),
        (2, n + 1, n),
        (3,),
    ]
    return pl.pallas_call(
        functools.partial(layer_kernel, n, tp, chunk),
        out_shape=jax.ShapeDtypeStruct((sub, width), bf16),
        in_specs=[pl.BlockSpec(memory_space=pltpu.VMEM)] * 7
        + [pl.BlockSpec(memory_space=pl.ANY)] * 3,
        out_specs=pl.BlockSpec(memory_space=pltpu.VMEM),
        scratch_shapes=[pltpu.VMEM(shape, dtype) for shape, dtype in shapes]
        + [pltpu.SemaphoreType.DMA(shape) for shape in sems],
        compiler_params=pltpu.CompilerParams(
            collective_id=0, has_side_effects=True, vmem_limit_bytes=60 * 1024 * 1024
        ),
    )(
        queries, keys, values, gates_t, residual, w_out, norm_gain[None, :],
        w_gate, w_up, w_down,
    )


def window(ff, n):
    return -(-ff // (n * 128)) * 128


def fits(mesh, shapes):
    residual, queries, gates, gate = shapes
    n, tp, grp = mesh.shape["sp"], mesh.shape["tp"], mesh.shape["grp"]
    ff = gate[1] // tp
    heads = gates[1] // tp
    head = queries[1] // gates[1]
    rows = residual[0] // (grp * n)
    return (
        grp == 2
        and n == 4
        and tp % 2 == 0
        and ff % 128 == 0
        and window(ff, n) * (n - 1) < ff
        and 128 % head == 0
        and (heads * head) % 128 == 0
        and rows % (16 * tp) == 0
        and rows * n * residual[1] <= 1 << 21
    )


def solution(mesh):
    in_specs = (
        P(("grp", "sp"), None),
        P(("grp", "sp"), "tp"),
        P(("grp", "sp"), "tp"),
        P(("grp", "sp"), "tp"),
        P(("grp", "sp"), "tp"),
        P("tp", None),
        P(),
        P("sp", "tp"),
        P("sp", "tp"),
        P("tp", "sp"),
    )
    out_specs = P(("grp", "sp", "tp"), None)

    def layer(*args):
        residual, queries, _, _, log_gates, _, _, w_gate, _, _ = args
        shapes = (residual.shape, queries.shape, log_gates.shape, w_gate.shape)
        chosen = fused_body if fits(mesh, shapes) else body
        return jax.shard_map(
            chosen, mesh=mesh, in_specs=in_specs, out_specs=out_specs, check_vma=False
        )(*args)

    return layer
```

```python
import functools
import math

import jax
import jax.numpy as jnp
from jax import lax
from jax.experimental import pallas as pl
from jax.experimental.pallas import tpu as pltpu
from jax.sharding import PartitionSpec as P


def normalize(rows_in, gain):
    floats = rows_in.astype(jnp.float32)
    scaled = floats * lax.rsqrt(jnp.mean(floats * floats, axis=-1, keepdims=True) + 1e-06)
    return (scaled * gain).astype(jnp.bfloat16)


def attend(queries, keys, values, log_gates):
    row_count = queries.shape[0]
    head_count = log_gates.shape[1]
    head_width = queries.shape[1] // head_count
    score_scale = head_width ** (-0.5)
    first_row = lax.axis_index("sp") * row_count
    query_heads = queries.reshape(row_count, head_count, head_width)
    query_gates = log_gates.T
    query_positions = first_row + jnp.arange(row_count, dtype=jnp.int32)
    initial = (
        jnp.full((head_count, row_count), -1e30, jnp.float32),
        jnp.zeros((head_count, row_count), jnp.float32),
        jnp.zeros((head_count, row_count, head_width), jnp.float32),
    )
    carried = initial
    key_piece = lax.all_gather(keys.astype(jnp.float32), "sp", axis=0, tiled=True).astype(
        jnp.bfloat16
    )
    value_piece = lax.all_gather(values.astype(jnp.float32), "sp", axis=0, tiled=True).astype(
        jnp.bfloat16
    )
    gate_piece = lax.all_gather(log_gates, "sp", axis=0, tiled=True)
    length = key_piece.shape[0]
    block_rows = math.gcd(length, 2048)
    block_count = length // block_rows
    key_blocks = key_piece.reshape(block_count, block_rows, head_count, head_width)
    value_blocks = value_piece.reshape(block_count, block_rows, head_count, head_width)
    gate_blocks = gate_piece.reshape(block_count, block_rows, head_count)
    offsets = jnp.arange(block_count, dtype=jnp.int32) * block_rows

    def one_block(state, inputs):
        current_key_block, value_block, gate_block, offset = inputs

        def work(current):
            running_max, running_sum, accumulated = current
            scores = (
                jnp.einsum(
                    "qhd,khd->hqk",
                    query_heads,
                    current_key_block,
                    preferred_element_type=jnp.float32,
                )
                * score_scale
            )
            scores = scores + query_gates[:, :, None] - gate_block.T[:, None, :]
            key_positions = offset + jnp.arange(block_rows, dtype=jnp.int32)
            causal = (query_positions[:, None] >= key_positions[None, :])[None]
            scores = jnp.where(causal, scores, -1e30)
            new_max = jnp.maximum(running_max, jnp.max(scores, axis=-1))
            weights = jnp.where(causal, jnp.exp(scores - new_max[:, :, None]), 0.0)
            rescale = jnp.exp(running_max - new_max)
            running_sum = running_sum * rescale + jnp.sum(weights, axis=-1)
            product = jnp.einsum(
                "hqk,khd->hqd",
                weights.astype(jnp.bfloat16),
                value_block,
                preferred_element_type=jnp.float32,
            )
            accumulated = accumulated * rescale[:, :, None] + product
            return (new_max, running_sum, accumulated)

        state = lax.cond(offset <= first_row + row_count - 1, work, lambda current: current, state)
        return (state, None)

    carried, _ = lax.scan(one_block, carried, (key_blocks, value_blocks, gate_blocks, offsets))
    running_max, running_sum, accumulated = carried
    attended = accumulated / running_sum[:, :, None]
    return (
        attended.transpose(1, 0, 2).reshape(row_count, head_count * head_width).astype(jnp.bfloat16)
    )


def body(residual, queries, keys, values, log_gates, w_out, norm_gain, w_gate, w_up, w_down):
    attended = attend(queries, keys, values, log_gates)
    row_count = attended.shape[0]
    per_device = row_count // lax.axis_size("tp")
    my_first = lax.axis_index("tp") * per_device
    projected = lax.psum(
        jnp.dot(attended, w_out, preferred_element_type=jnp.float32).astype(jnp.bfloat16), "tp"
    ).astype(jnp.float32)
    mixed_all = (residual.astype(jnp.float32) + projected).astype(jnp.bfloat16)
    normed_all = normalize(mixed_all, norm_gain)
    mixed = lax.dynamic_slice_in_dim(mixed_all, my_first, per_device, 0)
    gate_whole = lax.all_gather(w_gate, "sp", axis=0, tiled=True)
    up_whole = lax.all_gather(w_up, "sp", axis=0, tiled=True)
    down_whole = lax.all_gather(w_down, "sp", axis=1, tiled=True)
    gate_proj = jnp.dot(normed_all, gate_whole, preferred_element_type=jnp.float32)
    up_proj = jnp.dot(normed_all, up_whole, preferred_element_type=jnp.float32)
    hidden = (jax.nn.silu(gate_proj) * up_proj).astype(jnp.bfloat16)
    down_sum = lax.psum_scatter(
        jnp.dot(hidden, down_whole, preferred_element_type=jnp.float32).astype(jnp.bfloat16),
        "tp",
        scatter_dimension=0,
        tiled=True,
    ).astype(jnp.float32)
    summed = mixed.astype(jnp.float32) + 0.5 * down_sum
    scaled = summed * lax.rsqrt(jnp.mean(summed * summed, axis=-1, keepdims=True) + 1e-06)
    return scaled.astype(jnp.bfloat16)


MESH = pl.DeviceIdType.MESH
PIECES = 2
OPENING = (
    (("kv",), ("gu", 1), ("dn", 1), ("gu", 2, 3), ("prep",)),
    (("kv",), ("gu", 0), ("dn", 0), ("prep",), ("kv_in", 0), ("gu", 2, 3), ("fwd", 2)),
    (("kv",), ("gu", 1, 0), ("prep",), ("kv_in", 1), ("kv_in", 0), ("gu", 3), ("dn", 3), ("fwd", 3)),
    (("gu", 2), ("dn", 2), ("gu", 1, 0), ("prep",), ("kv_in", 2), ("kv_in", 1), ("kv_in", 0)),
)
EXCHANGE = (
    (
        ("own",), ("fwd", 1), ("hand", 0), ("fwd", 3), ("fwd", 2), ("fwd_dn", 1), ("in", 1),
        ("in", 2), ("hand", 1), ("in", 3), ("dn", 2, 3), ("hand", 2),
    ),
    (
        ("own",), ("fwd", 0), ("fwd", 3), ("hand", 1), ("fwd_dn", 0), ("in", 2), ("in", 0),
        ("dn", 2, 3), ("in", 3), ("hand", 0), ("hand", 2),
    ),
    (
        ("own",), ("fwd", 0), ("hand", 2), ("in", 3), ("dn", 1, 0), ("fwd_dn", 3), ("fwd", 1),
        ("in", 1), ("hand", 3), ("in", 0), ("hand", 1),
    ),
    (
        ("own",), ("fwd", 2), ("fwd", 0), ("hand", 3), ("fwd_dn", 2), ("in", 2), ("fwd", 1),
        ("in", 1), ("dn", 1, 0), ("hand", 2), ("in", 0), ("hand", 1),
    ),
)
LAST_ROWS = (3, 3, 0, 0)
STARTS = (2.0, 9.0, 16.5, 19.5)


def stage(n, s, j, e):
    lower = s < n // 2
    if j == s or (j > s) != lower or (e < n // 2) != lower:
        return 2
    if s in (0, n - 1):
        return 0 if e == s else 1
    return 1 if e in (0, n - 1) else 2


ROW_ORDER = ((0, 1, 2, 3), (1, 0, 2, 3), (2, 3, 1, 0), (3, 2, 1, 0))
COLUMN_ORDER = ((0, 1, 2, 3), (1, 0, 2, 3), (2, 3, 1, 0), (3, 2, 1, 0))


def line_tasks(n):
    wire, hop, add = 1.4, 1.8, 0.3
    base = (STARTS[1] + 2, STARTS[2] + 1, STARTS[3] + 1)
    term, clock = {}, [0.0] * n
    for s in range(n):
        link = 0.0
        for q, e in enumerate(COLUMN_ORDER[s]):
            for p in range(n):
                j = ROW_ORDER[s][p if q == 0 else n - 1 - p]
                link = max(link, STARTS[q] + (1.6 if q == 0 else 0.2) * p) + wire
                term[s, j, e] = link + hop
    waiting = {(s, j, e) for s in range(n) for j in range(n) for e in range(n) if j != s}
    arrival, links, tasks = {}, {}, [[] for _ in range(n)]
    while waiting:
        best = None
        for s, j, e in waiting:
            up = j > s
            behind = s - 1 if up else s + 1
            if 0 <= behind < n and (s, j, e) not in arrival:
                continue
            start = max(term[s, j, e], clock[s], base[stage(n, s, j, e)])
            start = max(start, arrival.get((s, j, e), 0.0))
            best = min(best or (start + 1, 0, 0), (start, -abs(j - s), (s, j, e)))
        start, _, (s, j, e) = best
        waiting.remove((s, j, e))
        tasks[s].append((j, e))
        up = j > s
        clock[s] = start + add
        links[s, up] = max(links.get((s, up), 0.0), start + add) + wire
        arrival[s + 1 if up else s - 1, j, e] = links[s, up] + hop
    for s in range(n):
        tasks[s] += [(s, e) for e in COLUMN_ORDER[s]]
    return tasks


def layer_kernel(
    n, tp, chunk,
    q_in, k_in, v_in, gt_in, residual_in, w_out_in, gain_in, wg_ref, wu_ref, wd_ref,
    out_ref,
    q_ref, k_ref, v_ref, gt_ref, residual_ref, w_out_ref, gain_ref,
    k_all, v_all, gt_all, att, proj, pc_buf, px_send, px_buf, mixed, normed,
    wg_all, wu_all, wd_all, hid, part, c_buf, x_send, x_buf, z_send, z_buf, total_ref,
    kv_sems, w_sems, y_sems, pc_sems, px_sems, nz_sems, nx_sems, nc_sems, c_sems, x_sems, z_sems, o_sems, i_sems,
):
    me = lax.axis_index("sp")
    t = lax.axis_index("tp")
    g = lax.axis_index("grp")
    x, c = t // 2, t % 2
    nx = tp // 2
    mate = x * 2 + (1 - c)
    rows = q_ref.shape[0]
    sub = rows // tp
    width = residual_ref.shape[1]
    heads = gt_ref.shape[0]
    head = q_ref.shape[1] // heads
    depth = wg_ref.shape[0]
    ff = wg_ref.shape[1]
    half = depth // 2
    dcols = wd_ref.shape[1]
    dhalf = dcols // 2
    GATE, UP, DOWN = range(3)

    def across(dx):
        return lax.rem(x + dx, nx)

    def per_me(work):
        for s in range(n):

            @pl.when(me == s)
            def _(s=s):
                work(s)

    def remote(src, dst, send_sem, recv_sem, target):
        return pltpu.make_async_remote_copy(
            src_ref=src, dst_ref=dst, send_sem=send_sem, recv_sem=recv_sem,
            device_id=target, device_id_type=MESH,
        )

    def arrived(slot, sems, *index):
        remote(slot, slot, sems.at[(0, *index)], sems.at[(1, *index)], {"tp": mate}).wait_recv()

    barrier = pltpu.get_barrier_semaphore()
    for d in range(1, n):
        pl.semaphore_signal(barrier, inc=1, device_id={"sp": lax.rem(me + d, n)}, device_id_type=MESH)
    for dx in range(1, nx):
        pl.semaphore_signal(
            barrier, inc=1, device_id={"tp": across(dx) * 2 + c}, device_id_type=MESH
        )
    pl.semaphore_signal(barrier, inc=1, device_id={"tp": mate}, device_id_type=MESH)
    pl.semaphore_signal(barrier, inc=1, device_id={"grp": 1 - g}, device_id_type=MESH)
    staged = [
        pltpu.make_async_copy(src, dst, i_sems.at[i])
        for i, (src, dst) in enumerate(
            (
                (k_in, k_ref), (v_in, v_ref), (gt_in, gt_ref), (q_in, q_ref),
                (w_out_in, w_out_ref), (residual_in, residual_ref), (gain_in, gain_ref),
            )
        )
    ]
    for copy in staged:
        copy.start()
    for copy in staged[:3]:
        copy.wait()
    pl.semaphore_wait(barrier, n - 1 + nx - 1 + 2)

    sent = [[] for _ in range(n)]

    def launch(s, make):
        make().start()
        sent[s].append(make)

    def kv_copy(s, o, i):
        own = (k_ref, v_ref, gt_ref)[i]
        held = (k_all, v_all, gt_all)[i].at[min(o, n - 2)]
        return remote(
            own if o == s else held, held, kv_sems.at[0, o, i], kv_sems.at[1, o, i], {"sp": s + 1}
        )

    def kv_send(s, o, i):
        launch(s, lambda: kv_copy(s, o, i))

    def kv_arrived(o, i):
        arrived((k_all, v_all, gt_all)[i].at[o], kv_sems, o, i)

    def size_of(j):
        return min(chunk, ff - j * chunk)

    def weight_slot(s, e, i, side):
        size = size_of(s)
        if i == DOWN:
            return wd_all.at[
                :size, pl.ds(pl.multiple_of(e * dcols + side * dhalf, 128), dhalf)
            ]
        held = (wg_all, wu_all)[i]
        return held.at[pl.ds(pl.multiple_of(e * depth + side * half, 16), half), :size]

    def weight_copy(s, j, i):
        place = pl.ds(j * chunk, size_of(j))
        if i == DOWN:
            src = wd_ref.at[place, pl.ds(pl.multiple_of(g * dhalf, 128), dhalf)]
        else:
            src = (wg_ref, wu_ref)[i].at[pl.ds(pl.multiple_of(g * half, 16), half), place]
        return remote(
            src, weight_slot(j, s, i, g), w_sems.at[0, j, i], w_sems.at[1, s, i], {"sp": j}
        )

    def weights(s, targets, pieces):
        for j in targets:
            for i in pieces:
                launch(s, lambda j=j, i=i: weight_copy(s, j, i))

    def relay_weights(s, e, pieces):
        for i in pieces:
            slot = weight_slot(s, e, i, g)
            arrived(slot, w_sems, e, i)

            def make(i=i):
                place = weight_slot(s, e, i, g)
                return remote(
                    place, place, y_sems.at[0, e, i], y_sems.at[1, e, i], {"grp": 1 - g}
                )

            launch(s, make)

    def weights_there(s, e, pieces):
        for i in pieces:
            arrived(weight_slot(s, e, i, 1 - g), y_sems, e, i)

    def own_copies(s):
        size = size_of(s)
        mine = pl.ds(s * chunk, size)
        return (
            pltpu.make_async_copy(
                wg_ref.at[:, mine], wg_all.at[pl.ds(s * depth, depth), :size], o_sems.at[0]
            ),
            pltpu.make_async_copy(
                wu_ref.at[:, mine], wu_all.at[pl.ds(s * depth, depth), :size], o_sems.at[1]
            ),
            pltpu.make_async_copy(
                wd_ref.at[mine, :], wd_all.at[:size, pl.ds(s * dcols, dcols)], o_sems.at[2]
            ),
        )

    span = width // PIECES

    def row_slot(o, owner, k):
        return normed.at[o, owner, :, k * span : (k + 1) * span]

    def pass_rows(s, o, k):
        for way, j in ((0, s + 1), (1, s - 1)):
            if 0 <= j < n and (o == s or (o < s) == (way == 0)):

                def make(way=way, j=j):
                    slot = row_slot(o, t, k)
                    return remote(
                        slot, slot, nz_sems.at[way, o, k], nz_sems.at[2, o, k], {"sp": j}
                    )

                launch(s, make)

    def spread_rows(s, o, k):
        def to_mate():
            slot = row_slot(o, t, k)
            return remote(slot, slot, nc_sems.at[0, o, 0, k], nc_sems.at[1, o, 0, k], {"tp": mate})

        for dx in range(1, nx):

            def over(dx=dx):
                slot = row_slot(o, t, k)
                return remote(
                    slot, slot, nx_sems.at[0, o, dx, k], nx_sems.at[1, o, dx, k],
                    {"tp": across(dx) * 2 + c},
                )

            launch(s, over)
        launch(s, to_mate)

    def rows_in(s, *origins):
        for o in origins:
            for k in range(PIECES):
                slot = row_slot(o, t, k)
                remote(
                    slot, slot, nz_sems.at[0, o, k], nz_sems.at[2, o, k], {"tp": mate}
                ).wait_recv()
                pass_rows(s, o, k)
                spread_rows(s, o, k)

    def hand_over(s, *origins):
        for o in origins:
            for k in range(PIECES):
                for dx in range(1, nx):
                    owner = lax.rem(x + nx - dx, nx) * 2 + c
                    arrived(row_slot(o, owner, k), nx_sems, o, dx, k)

                    def make(o=o, dx=dx, k=k):
                        slot = row_slot(o, lax.rem(x + nx - dx, nx) * 2 + c, k)
                        return remote(
                            slot, slot, nc_sems.at[0, o, dx, k], nc_sems.at[1, o, dx, k],
                            {"tp": mate},
                        )

                    launch(s, make)

    def rows_ready(o):
        for k in range(PIECES):
            for dx in range(nx):
                owner = lax.rem(x + nx - dx, nx) * 2 + 1 - c
                arrived(row_slot(o, owner, k), nc_sems, o, dx, k)

    def kv_in(s, o):
        for i in range(3):
            kv_arrived(o, i)
            if s < n - 1:
                kv_send(s, o, i)

    def kv_out(s):
        if s < n - 1:
            for i in range(3):
                kv_send(s, s, i)

    def prepare(s):
        for copy in own_copies(s):
            copy.start()
        size = size_of(s)
        if size < chunk:
            wg_all[:, size:] = jnp.zeros((n * depth, chunk - size), jnp.bfloat16)
            wu_all[:, size:] = jnp.zeros((n * depth, chunk - size), jnp.bfloat16)
            wd_all[size:, :] = jnp.zeros((chunk - size, n * dcols), jnp.bfloat16)
        for o in range(s, n - 1):
            k_all[o] = jnp.zeros_like(k_ref)
            v_all[o] = jnp.zeros_like(v_ref)
            gt_all[o] = jnp.zeros_like(gt_ref)

    def own_rows(s):
        for k in range(PIECES):
            pass_rows(s, s, k)
            spread_rows(s, s, k)

    steps = {
        "kv": kv_out,
        "kv_in": kv_in,
        "own": own_rows,
        "gu": lambda s, *to: weights(s, to, (GATE, UP)),
        "dn": lambda s, *to: weights(s, to, (DOWN,)),
        "in": lambda s, *origins: rows_in(s, *origins),
        "hand": lambda s, *origins: hand_over(s, *origins),
        "fwd": lambda s, e: relay_weights(s, e, (GATE, UP)),
        "fwd_dn": lambda s, e: relay_weights(s, e, (DOWN,)),
        "prep": prepare,
    }

    def follow(s, plan):
        for name, *where in plan:
            steps[name](s, *where)

    per_me(lambda s: follow(s, OPENING[s]))

    for copy in staged[3:]:
        copy.wait()
    pair = 128 // head
    lane = lax.broadcasted_iota(jnp.int32, (rows, 128), 1)
    causal = lax.broadcasted_iota(jnp.int32, (rows, rows), 0) >= lax.broadcasted_iota(
        jnp.int32, (rows, rows), 1
    )
    contract = (((1,), (1,)), ((), ()))
    filler = -heads % 8
    gates = gt_ref[...]
    if filler:
        gates = jnp.concatenate([gates, jnp.zeros((filler, rows), jnp.float32)], axis=0)
    gates = gates.T
    for p in range(heads // pair):
        cols = slice(p * 128, (p + 1) * 128)
        q_pair = q_ref[:, cols]
        joined = jnp.zeros((rows, 128), jnp.float32)
        for i in range(pair):
            h = p * pair + i
            inside = (lane >= i * head) & (lane < (i + 1) * head)
            q_head = jnp.where(inside, q_pair, jnp.zeros_like(q_pair))
            g_query = gates[:, h : h + 1]
            scores = []
            for o in range(n):
                k_pair = k_ref[:, cols] if o == n - 1 else k_all[o, :, cols]
                g_key = gt_ref[h : h + 1, :] if o == n - 1 else gt_all[o, h : h + 1, :]
                score = (
                    lax.dot_general(q_head, k_pair, contract, preferred_element_type=jnp.float32)
                    * head ** (-0.5)
                    + g_query
                    - g_key
                )
                allowed = causal if o == n - 1 else (jnp.zeros((rows, rows), jnp.int32) + me) > o
                scores.append(jnp.where(allowed, score, -1e30))
            peak = functools.reduce(
                jnp.maximum, [jnp.max(score, axis=-1, keepdims=True) for score in scores]
            )
            total = jnp.zeros((rows, 1), jnp.float32)
            summed = jnp.zeros((rows, 128), jnp.float32)
            for o in range(n):
                v_pair = v_ref[:, cols] if o == n - 1 else v_all[o, :, cols]
                weight = jnp.exp(scores[o] - peak)
                total += jnp.sum(weight, axis=-1, keepdims=True)
                summed += jnp.dot(
                    weight.astype(jnp.bfloat16), v_pair, preferred_element_type=jnp.float32
                )
            joined = jnp.where(inside, summed / total, joined)
        att[:, cols] = joined.astype(jnp.bfloat16)

    for k in range(width // 512):
        cols = slice(k * 512, (k + 1) * 512)
        proj[:, cols] = jnp.dot(
            att[...], w_out_ref[:, cols], preferred_element_type=jnp.float32
        ).astype(jnp.bfloat16)

    def block(index):
        return pl.ds(pl.multiple_of(index * sub, sub), sub)

    pc = [
        remote(
            proj.at[block(across(dx) * 2 + 1 - c)], pc_buf.at[dx],
            pc_sems.at[0, dx], pc_sems.at[1, dx], {"tp": mate},
        )
        for dx in range(nx)
    ]
    for dx in (*range(1, nx), 0):
        pc[dx].start()
    px = [
        remote(
            px_send.at[dx], px_buf.at[dx], px_sems.at[0, dx], px_sems.at[1, dx],
            {"tp": across(dx) * 2 + c},
        )
        for dx in range(nx)
    ]
    for dx in range(1, nx):
        pc[dx].wait_recv()
        px_send[dx] = (
            proj[block(across(dx) * 2 + c), :].astype(jnp.float32) + pc_buf[dx].astype(jnp.float32)
        ).astype(jnp.bfloat16)
        px[dx].start()
    pc[0].wait_recv()
    acc = proj[block(t), :].astype(jnp.float32) + pc_buf[0].astype(jnp.float32)
    for dx in range(1, nx):
        px[dx].wait_recv()
        acc += px_buf[dx].astype(jnp.float32)
    mix = (residual_ref[block(t), :].astype(jnp.float32) + acc).astype(jnp.bfloat16)
    mixed[...] = mix
    floats = mix.astype(jnp.float32)
    scale = lax.rsqrt(jnp.mean(floats * floats, axis=-1, keepdims=True) + 1e-06)
    normed[me, t] = (floats * scale * gain_ref[...]).astype(jnp.bfloat16)

    def exchange(s):
        follow(s, EXCHANGE[s])
        for e in range(n):
            if e != s:
                weights_there(s, e, (GATE, UP))
        for copy in own_copies(s):
            copy.wait()

    per_me(exchange)

    def span_of(e):
        return pl.ds(e * dcols if isinstance(e, int) else pl.multiple_of(e * dcols, 128), dcols)

    def c_copy(j, e):
        return remote(
            part.at[j, :, 1 - c, :, span_of(e)], c_buf.at[j, :, :, span_of(e)],
            c_sems.at[0, j, e], c_sems.at[1, j, e], {"tp": mate},
        )

    def x_copy(j, dx, e):
        return remote(
            x_send.at[j, dx, :, span_of(e)], x_buf.at[j, dx, :, span_of(e)],
            x_sems.at[0, j, dx, e], x_sems.at[1, j, dx, e], {"tp": across(dx) * 2 + c},
        )

    high = me // (n // 2)
    row_order = [me, me + 1 - 2 * lax.rem(me, 2), n // 2 - high, (n - 1) * (1 - high)]
    column_order = row_order

    def down_part(j, e):
        product = jnp.dot(
            hid[j], wd_all[:, span_of(e)], preferred_element_type=jnp.float32
        ).astype(jnp.bfloat16)
        part[j, :, :, :, span_of(e)] = product.reshape(nx, 2, sub, dcols)
        c_copy(j, e).start()

    def over_x(j, e):
        c_copy(j, e).wait_recv()
        for dx in range(1, nx):
            x_send[j, dx, :, span_of(e)] = (
                part[j, across(dx), c, :, span_of(e)].astype(jnp.float32)
                + c_buf[j, across(dx), :, span_of(e)].astype(jnp.float32)
            ).astype(jnp.bfloat16)
            x_copy(j, dx, e).start()

    def down_arrived(s, e):
        if (("fwd_dn", e)) not in EXCHANGE[s]:
            relay_weights(s, e, (DOWN,))

    def down_there(s, e):
        weights_there(s, e, (DOWN,))

    for k, j in enumerate(row_order):
        if k == 2:
            per_me(lambda s: hand_over(s, LAST_ROWS[s]))
        per_me(lambda s: rows_ready(ROW_ORDER[s][k]))
        piece = normed[j].reshape(rows, width)
        gate = jnp.dot(piece, wg_all[...], preferred_element_type=jnp.float32)
        up = jnp.dot(piece, wu_all[...], preferred_element_type=jnp.float32)
        hid[j] = (gate / (1.0 + jnp.exp(-gate)) * up).astype(jnp.bfloat16)
        down_part(j, column_order[0])
        if k:
            over_x(row_order[k - 1], column_order[0])
    over_x(row_order[-1], column_order[0])

    def local_sum(j, e):
        acc = part[j, x, c, :, span_of(e)].astype(jnp.float32) + c_buf[
            j, x, :, span_of(e)
        ].astype(jnp.float32)
        for dx in range(1, nx):
            x_copy(j, dx, e).wait_recv()
            acc += x_buf[j, dx, :, span_of(e)].astype(jnp.float32)
        return acc

    def z_in(slot, e):
        place = z_buf.at[slot, :, span_of(e)]
        remote(
            place, place, z_sems.at[0, slot, e], z_sems.at[1, slot, e], {"tp": mate}
        ).wait_recv()
        return z_buf[slot, :, span_of(e)].astype(jnp.float32)

    def over_z(s, j, e):
        acc = local_sum(j, e)
        to = s + 1 if j > s else s - 1
        behind = s - 1 if j > s else s + 1
        if 0 <= behind < n:
            acc += z_in(j, e)
        z_send[j, :, span_of(e)] = acc.astype(jnp.bfloat16)
        slot = n if to == j and j < s else j

        def make():
            return remote(
                z_send.at[j, :, span_of(e)], z_buf.at[slot, :, span_of(e)],
                z_sems.at[0, j, e], z_sems.at[1, slot, e], {"sp": to},
            )

        launch(s, make)

    def finish(s, e):
        acc = local_sum(s, e)
        if s > 0:
            acc += z_in(s, e)
        if s < n - 1:
            acc += z_in(n, e)
        total_ref[:, span_of(e)] = mixed[:, span_of(e)].astype(jnp.float32) + 0.5 * acc

    order = line_tasks(n)

    def along(s, due):
        for j, e in order[s]:
            if stage(n, s, j, e) == due:
                if j == s:
                    finish(s, e)
                else:
                    over_z(s, j, e)

    for q in range(1, n):
        if q == 1:
            per_me(lambda s: down_arrived(s, COLUMN_ORDER[s][1]))
        per_me(lambda s: down_there(s, COLUMN_ORDER[s][q]))
        for j in row_order[::-1]:
            down_part(j, column_order[q])
        for j in row_order[::-1]:
            over_x(j, column_order[q])
        if q == 1:
            per_me(lambda s: [down_arrived(s, e) for e in COLUMN_ORDER[s][2:]])
        if q < 3:
            per_me(lambda s: along(s, q - 1))

    per_me(lambda s: along(s, 2))
    summed = total_ref[...]
    scale = lax.rsqrt(jnp.mean(summed * summed, axis=-1, keepdims=True) + 1e-06)
    out_ref[...] = (summed * scale).astype(jnp.bfloat16)

    for copy in pc:
        copy.wait_send()
    for dx in range(1, nx):
        px[dx].wait_send()
    for e in range(n):
        for j in range(n):
            c_copy(j, e).wait_send()
            for dx in range(1, nx):
                x_copy(j, dx, e).wait_send()

    def all_sent(s):
        for make in sent[s]:
            make().wait_send()

    per_me(all_sent)


def fused_body(residual, queries, keys, values, log_gates, w_out, norm_gain, w_gate, w_up, w_down):
    n, tp = lax.axis_size("sp"), lax.axis_size("tp")
    rows, width = residual.shape
    sub = rows // tp
    nx = tp // 2
    depth, ff = w_gate.shape
    dcols = w_down.shape[1]
    chunk = window(ff, n)
    gates_t = log_gates.T
    bf16, f32 = jnp.bfloat16, jnp.float32
    shapes = [
        (queries.shape, bf16),
        (keys.shape, bf16),
        (values.shape, bf16),
        (gates_t.shape, f32),
        (residual.shape, bf16),
        (w_out.shape, bf16),
        ((1, width), f32),
        ((n - 1, *keys.shape), bf16),
        ((n - 1, *values.shape), bf16),
        ((n - 1, *gates_t.shape), f32),
        (queries.shape, bf16),
        ((rows, width), bf16),
        ((nx, sub, width), bf16),
        ((nx, sub, width), bf16),
        ((nx, sub, width), bf16),
        ((sub, width), bf16),
        ((n, tp, sub, width), bf16),
        ((n * depth, chunk), bf16),
        ((n * depth, chunk), bf16),
        ((chunk, n * dcols), bf16),
        ((n, rows, chunk), bf16),
        ((n, nx, 2, sub, width), bf16),
        ((n, nx, sub, width), bf16),
        ((n, nx, sub, width), bf16),
        ((n, nx, sub, width), bf16),
        ((n, sub, width), bf16),
        ((n + 1, sub, width), bf16),
        ((sub, width), f32),
    ]
    sems = [
        (2, n, 3),
        (2, n, 3),
        (2, n, 3),
        (2, nx),
        (2, nx),
        (3, n, PIECES),
        (2, n, nx, PIECES),
        (2, n, nx, PIECES),
        (2, n, n),
        (2, n, nx, n),
        (2, n + 1, n),
        (3,),
        (7,),
    ]
    return pl.pallas_call(
        functools.partial(layer_kernel, n, tp, chunk),
        out_shape=jax.ShapeDtypeStruct((sub, width), bf16),
        in_specs=[pl.BlockSpec(memory_space=pl.ANY)] * 10,
        out_specs=pl.BlockSpec(memory_space=pltpu.VMEM),
        scratch_shapes=[pltpu.VMEM(shape, dtype) for shape, dtype in shapes]
        + [pltpu.SemaphoreType.DMA(shape) for shape in sems],
        compiler_params=pltpu.CompilerParams(
            collective_id=0, has_side_effects=True, vmem_limit_bytes=60 * 1024 * 1024
        ),
    )(
        queries, keys, values, gates_t, residual, w_out, norm_gain[None, :],
        w_gate, w_up, w_down,
    )


def window(ff, n):
    return -(-ff // (n * 128)) * 128


def fits(mesh, shapes):
    residual, queries, gates, gate = shapes
    n, tp, grp = mesh.shape["sp"], mesh.shape["tp"], mesh.shape["grp"]
    ff = gate[1] // tp
    heads = gates[1] // tp
    head = queries[1] // gates[1]
    rows = residual[0] // (grp * n)
    return (
        grp == 2
        and n == 4
        and tp % 2 == 0
        and ff % 128 == 0
        and window(ff, n) * (n - 1) < ff
        and 128 % head == 0
        and (heads * head) % 128 == 0
        and rows % (16 * tp) == 0
        and rows * n * residual[1] <= 1 << 21
    )


def solution(mesh):
    in_specs = (
        P(("grp", "sp"), None),
        P(("grp", "sp"), "tp"),
        P(("grp", "sp"), "tp"),
        P(("grp", "sp"), "tp"),
        P(("grp", "sp"), "tp"),
        P("tp", None),
        P(),
        P("sp", "tp"),
        P("sp", "tp"),
        P("tp", "sp"),
    )
    out_specs = P(("grp", "sp", "tp"), None)

    def layer(*args):
        residual, queries, _, _, log_gates, _, _, w_gate, _, _ = args
        shapes = (residual.shape, queries.shape, log_gates.shape, w_gate.shape)
        chosen = fused_body if fits(mesh, shapes) else body
        return jax.shard_map(
            chosen, mesh=mesh, in_specs=in_specs, out_specs=out_specs, check_vma=False
        )(*args)

    return layer
```

```python
import functools
import math

import jax
import jax.numpy as jnp
from jax import lax
from jax.experimental import pallas as pl
from jax.experimental.pallas import tpu as pltpu
from jax.sharding import PartitionSpec as P


def normalize(rows_in, gain):
    floats = rows_in.astype(jnp.float32)
    scaled = floats * lax.rsqrt(jnp.mean(floats * floats, axis=-1, keepdims=True) + 1e-06)
    return (scaled * gain).astype(jnp.bfloat16)


def attend(queries, keys, values, log_gates):
    row_count = queries.shape[0]
    head_count = log_gates.shape[1]
    head_width = queries.shape[1] // head_count
    score_scale = head_width ** (-0.5)
    first_row = lax.axis_index("sp") * row_count
    query_heads = queries.reshape(row_count, head_count, head_width)
    query_gates = log_gates.T
    query_positions = first_row + jnp.arange(row_count, dtype=jnp.int32)
    initial = (
        jnp.full((head_count, row_count), -1e30, jnp.float32),
        jnp.zeros((head_count, row_count), jnp.float32),
        jnp.zeros((head_count, row_count, head_width), jnp.float32),
    )
    carried = initial
    key_piece = lax.all_gather(keys.astype(jnp.float32), "sp", axis=0, tiled=True).astype(
        jnp.bfloat16
    )
    value_piece = lax.all_gather(values.astype(jnp.float32), "sp", axis=0, tiled=True).astype(
        jnp.bfloat16
    )
    gate_piece = lax.all_gather(log_gates, "sp", axis=0, tiled=True)
    length = key_piece.shape[0]
    block_rows = math.gcd(length, 2048)
    block_count = length // block_rows
    key_blocks = key_piece.reshape(block_count, block_rows, head_count, head_width)
    value_blocks = value_piece.reshape(block_count, block_rows, head_count, head_width)
    gate_blocks = gate_piece.reshape(block_count, block_rows, head_count)
    offsets = jnp.arange(block_count, dtype=jnp.int32) * block_rows

    def one_block(state, inputs):
        current_key_block, value_block, gate_block, offset = inputs

        def work(current):
            running_max, running_sum, accumulated = current
            scores = (
                jnp.einsum(
                    "qhd,khd->hqk",
                    query_heads,
                    current_key_block,
                    preferred_element_type=jnp.float32,
                )
                * score_scale
            )
            scores = scores + query_gates[:, :, None] - gate_block.T[:, None, :]
            key_positions = offset + jnp.arange(block_rows, dtype=jnp.int32)
            causal = (query_positions[:, None] >= key_positions[None, :])[None]
            scores = jnp.where(causal, scores, -1e30)
            new_max = jnp.maximum(running_max, jnp.max(scores, axis=-1))
            weights = jnp.where(causal, jnp.exp(scores - new_max[:, :, None]), 0.0)
            rescale = jnp.exp(running_max - new_max)
            running_sum = running_sum * rescale + jnp.sum(weights, axis=-1)
            product = jnp.einsum(
                "hqk,khd->hqd",
                weights.astype(jnp.bfloat16),
                value_block,
                preferred_element_type=jnp.float32,
            )
            accumulated = accumulated * rescale[:, :, None] + product
            return (new_max, running_sum, accumulated)

        state = lax.cond(offset <= first_row + row_count - 1, work, lambda current: current, state)
        return (state, None)

    carried, _ = lax.scan(one_block, carried, (key_blocks, value_blocks, gate_blocks, offsets))
    running_max, running_sum, accumulated = carried
    attended = accumulated / running_sum[:, :, None]
    return (
        attended.transpose(1, 0, 2).reshape(row_count, head_count * head_width).astype(jnp.bfloat16)
    )


def body(residual, queries, keys, values, log_gates, w_out, norm_gain, w_gate, w_up, w_down):
    attended = attend(queries, keys, values, log_gates)
    row_count = attended.shape[0]
    per_device = row_count // lax.axis_size("tp")
    my_first = lax.axis_index("tp") * per_device
    projected = lax.psum(
        jnp.dot(attended, w_out, preferred_element_type=jnp.float32).astype(jnp.bfloat16), "tp"
    ).astype(jnp.float32)
    mixed_all = (residual.astype(jnp.float32) + projected).astype(jnp.bfloat16)
    normed_all = normalize(mixed_all, norm_gain)
    mixed = lax.dynamic_slice_in_dim(mixed_all, my_first, per_device, 0)
    gate_whole = lax.all_gather(w_gate, "sp", axis=0, tiled=True)
    up_whole = lax.all_gather(w_up, "sp", axis=0, tiled=True)
    down_whole = lax.all_gather(w_down, "sp", axis=1, tiled=True)
    gate_proj = jnp.dot(normed_all, gate_whole, preferred_element_type=jnp.float32)
    up_proj = jnp.dot(normed_all, up_whole, preferred_element_type=jnp.float32)
    hidden = (jax.nn.silu(gate_proj) * up_proj).astype(jnp.bfloat16)
    down_sum = lax.psum_scatter(
        jnp.dot(hidden, down_whole, preferred_element_type=jnp.float32).astype(jnp.bfloat16),
        "tp",
        scatter_dimension=0,
        tiled=True,
    ).astype(jnp.float32)
    summed = mixed.astype(jnp.float32) + 0.5 * down_sum
    scaled = summed * lax.rsqrt(jnp.mean(summed * summed, axis=-1, keepdims=True) + 1e-06)
    return scaled.astype(jnp.bfloat16)


MESH = pl.DeviceIdType.MESH
PIECES = 2
OPENING = (
    (("kv",), ("gu", 1), ("dn", 1), ("gu", 2, 3), ("prep",)),
    (("kv",), ("gu", 0), ("dn", 0), ("prep",), ("kv_in", 0), ("gu", 2, 3), ("fwd", 2)),
    (("kv",), ("gu", 1, 0), ("prep",), ("kv_in", 1), ("kv_in", 0), ("gu", 3), ("dn", 3), ("fwd", 3)),
    (("gu", 2), ("dn", 2), ("gu", 1, 0), ("prep",), ("kv_in", 2), ("kv_in", 1), ("kv_in", 0)),
)
EXCHANGE = (
    (
        ("own",), ("fwd", 1), ("hand", 0), ("fwd", 3), ("fwd", 2), ("fwd_dn", 1), ("in", 1),
        ("in", 2), ("hand", 1), ("in", 3), ("dn", 2, 3), ("hand", 2),
    ),
    (
        ("own",), ("fwd", 0), ("fwd", 3), ("hand", 1), ("fwd_dn", 0), ("in", 2), ("in", 0),
        ("dn", 2, 3), ("in", 3), ("hand", 0), ("hand", 2),
    ),
    (
        ("own",), ("fwd", 0), ("hand", 2), ("in", 3), ("dn", 1, 0), ("fwd_dn", 3), ("fwd", 1),
        ("in", 1), ("hand", 3), ("in", 0), ("hand", 1),
    ),
    (
        ("own",), ("fwd", 2), ("fwd", 0), ("hand", 3), ("fwd_dn", 2), ("in", 2), ("fwd", 1),
        ("in", 1), ("dn", 1, 0), ("hand", 2), ("in", 0), ("hand", 1),
    ),
)
LATE = ((("hand", 3),), (("hand", 3),), (("hand", 0),), (("hand", 0),))
STARTS = (2.0, 9.0, 16.5, 19.5)


def direct(n, up, e):
    return e == (n - 1 if up else 0)


def stage(n, s, j, e):
    lower = s < n // 2
    if j == s or (j > s) != lower or (e < n // 2) != lower:
        return 2
    if s in (0, n - 1):
        return 0 if e == s else 1
    return 1 if e in (0, n - 1) else 2


ROW_ORDER = ((0, 1, 2, 3), (1, 0, 2, 3), (2, 3, 1, 0), (3, 2, 1, 0))
COLUMN_ORDER = ((0, 1, 2, 3), (1, 0, 2, 3), (2, 3, 1, 0), (3, 2, 1, 0))


def line_tasks(n):
    wire, hop, add = 1.4, 3.5, 0.3
    base = (STARTS[1] + 2, STARTS[2] + 1, STARTS[3] + 1)
    term, clock = {}, [0.0] * n
    for s in range(n):
        link = 0.0
        for q, e in enumerate(COLUMN_ORDER[s]):
            for p in range(n):
                j = ROW_ORDER[s][p if q == 0 else n - 1 - p]
                link = max(link, STARTS[q] + (1.6 if q == 0 else 0.2) * p) + wire
                term[s, j, e] = link + hop
    waiting = {(s, j, e) for s in range(n) for j in range(n) for e in range(n) if j != s}
    arrival, links, tasks = {}, {}, [[] for _ in range(n)]
    while waiting:
        best = None
        for s, j, e in waiting:
            up = j > s
            behind = s - 1 if up else s + 1
            if 0 <= behind < n and (s, j, e) not in arrival and not direct(n, up, e):
                continue
            start = max(term[s, j, e], clock[s], base[stage(n, s, j, e)])
            start = max(start, arrival.get((s, j, e), 0.0))
            best = min(best or (start + 1, 0, 0), (start, -abs(j - s), (s, j, e)))
        start, _, (s, j, e) = best
        waiting.remove((s, j, e))
        tasks[s].append((j, e))
        up = j > s
        clock[s] = start + add
        links[s, up] = max(links.get((s, up), 0.0), start + add) + wire
        if not direct(n, up, e):
            arrival[s + 1 if up else s - 1, j, e] = links[s, up] + hop
    for s in range(n):
        tasks[s] += [(s, e) for e in COLUMN_ORDER[s]]
    return tasks


def layer_kernel(
    n, tp, chunk,
    q_in, k_in, v_in, gt_in, residual_in, w_out_in, gain_in, wg_ref, wu_ref, wd_ref,
    out_ref,
    q_ref, k_ref, v_ref, gt_ref, residual_ref, w_out_ref, gain_ref,
    k_all, v_all, gt_all, att, proj, pc_buf, px_send, px_buf, mixed, normed,
    wg_all, wu_all, wd_all, hid, part, c_buf, x_send, x_buf, z_send, z_buf, total_ref,
    kv_sems, w_sems, y_sems, pc_sems, px_sems, nz_sems, nx_sems, nc_sems, c_sems, x_sems, z_sems, o_sems, i_sems,
):
    me = lax.axis_index("sp")
    t = lax.axis_index("tp")
    g = lax.axis_index("grp")
    x, c = t // 2, t % 2
    nx = tp // 2
    mate = x * 2 + (1 - c)
    rows = q_ref.shape[0]
    sub = rows // tp
    width = residual_ref.shape[1]
    heads = gt_ref.shape[0]
    head = q_ref.shape[1] // heads
    depth = wg_ref.shape[0]
    ff = wg_ref.shape[1]
    half = depth // 2
    dcols = wd_ref.shape[1]
    dhalf = dcols // 2
    GATE, UP, DOWN = range(3)

    def across(dx):
        return lax.rem(x + dx, nx)

    def per_me(work):
        for s in range(n):

            @pl.when(me == s)
            def _(s=s):
                work(s)

    def remote(src, dst, send_sem, recv_sem, target):
        return pltpu.make_async_remote_copy(
            src_ref=src, dst_ref=dst, send_sem=send_sem, recv_sem=recv_sem,
            device_id=target, device_id_type=MESH,
        )

    def arrived(slot, sems, *index):
        remote(slot, slot, sems.at[(0, *index)], sems.at[(1, *index)], {"tp": mate}).wait_recv()

    barrier = pltpu.get_barrier_semaphore()
    for d in range(1, n):
        pl.semaphore_signal(barrier, inc=1, device_id={"sp": lax.rem(me + d, n)}, device_id_type=MESH)
    for dx in range(1, nx):
        pl.semaphore_signal(
            barrier, inc=1, device_id={"tp": across(dx) * 2 + c}, device_id_type=MESH
        )
    pl.semaphore_signal(barrier, inc=1, device_id={"tp": mate}, device_id_type=MESH)
    pl.semaphore_signal(barrier, inc=1, device_id={"grp": 1 - g}, device_id_type=MESH)
    staged = [
        pltpu.make_async_copy(src, dst, i_sems.at[i])
        for i, (src, dst) in enumerate(
            (
                (k_in, k_ref), (v_in, v_ref), (gt_in, gt_ref), (q_in, q_ref),
                (w_out_in, w_out_ref), (residual_in, residual_ref), (gain_in, gain_ref),
            )
        )
    ]
    for copy in staged:
        copy.start()
    for copy in staged[:3]:
        copy.wait()
    pl.semaphore_wait(barrier, n - 1 + nx - 1 + 2)

    sent = [[] for _ in range(n)]

    def launch(s, make):
        make().start()
        sent[s].append(make)

    def kv_copy(s, o, i):
        own = (k_ref, v_ref, gt_ref)[i]
        held = (k_all, v_all, gt_all)[i].at[min(o, n - 2)]
        return remote(
            own if o == s else held, held, kv_sems.at[0, o, i], kv_sems.at[1, o, i], {"sp": s + 1}
        )

    def kv_send(s, o, i):
        launch(s, lambda: kv_copy(s, o, i))

    def kv_arrived(o, i):
        arrived((k_all, v_all, gt_all)[i].at[o], kv_sems, o, i)

    def size_of(j):
        return min(chunk, ff - j * chunk)

    def weight_slot(s, e, i, side):
        size = size_of(s)
        if i == DOWN:
            return wd_all.at[
                :size, pl.ds(pl.multiple_of(e * dcols + side * dhalf, 128), dhalf)
            ]
        held = (wg_all, wu_all)[i]
        return held.at[pl.ds(pl.multiple_of(e * depth + side * half, 16), half), :size]

    def weight_copy(s, j, i):
        place = pl.ds(j * chunk, size_of(j))
        if i == DOWN:
            src = wd_ref.at[place, pl.ds(pl.multiple_of(g * dhalf, 128), dhalf)]
        else:
            src = (wg_ref, wu_ref)[i].at[pl.ds(pl.multiple_of(g * half, 16), half), place]
        return remote(
            src, weight_slot(j, s, i, g), w_sems.at[0, j, i], w_sems.at[1, s, i], {"sp": j}
        )

    def weights(s, targets, pieces):
        for j in targets:
            for i in pieces:
                launch(s, lambda j=j, i=i: weight_copy(s, j, i))

    def relay_weights(s, e, pieces):
        for i in pieces:
            slot = weight_slot(s, e, i, g)
            arrived(slot, w_sems, e, i)

            def make(i=i):
                place = weight_slot(s, e, i, g)
                return remote(
                    place, place, y_sems.at[0, e, i], y_sems.at[1, e, i], {"grp": 1 - g}
                )

            launch(s, make)

    def weights_there(s, e, pieces):
        for i in pieces:
            arrived(weight_slot(s, e, i, 1 - g), y_sems, e, i)

    def own_copies(s):
        size = size_of(s)
        mine = pl.ds(s * chunk, size)
        return (
            pltpu.make_async_copy(
                wg_ref.at[:, mine], wg_all.at[pl.ds(s * depth, depth), :size], o_sems.at[0]
            ),
            pltpu.make_async_copy(
                wu_ref.at[:, mine], wu_all.at[pl.ds(s * depth, depth), :size], o_sems.at[1]
            ),
            pltpu.make_async_copy(
                wd_ref.at[mine, :], wd_all.at[:size, pl.ds(s * dcols, dcols)], o_sems.at[2]
            ),
        )

    span = width // PIECES

    def row_slot(o, owner, k):
        return normed.at[o, owner, :, k * span : (k + 1) * span]

    def pass_rows(s, o, k):
        for way, j in ((0, s + 1), (1, s - 1)):
            if 0 <= j < n and (o == s or (o < s) == (way == 0)):

                def make(way=way, j=j):
                    slot = row_slot(o, t, k)
                    return remote(
                        slot, slot, nz_sems.at[way, o, k], nz_sems.at[2, o, k], {"sp": j}
                    )

                launch(s, make)

    def spread_rows(s, o, k):
        def to_mate():
            slot = row_slot(o, t, k)
            return remote(slot, slot, nc_sems.at[0, o, 0, k], nc_sems.at[1, o, 0, k], {"tp": mate})

        for dx in range(1, nx):

            def over(dx=dx):
                slot = row_slot(o, t, k)
                return remote(
                    slot, slot, nx_sems.at[0, o, dx, k], nx_sems.at[1, o, dx, k],
                    {"tp": across(dx) * 2 + c},
                )

            launch(s, over)
        launch(s, to_mate)

    def rows_in(s, *origins):
        for o in origins:
            for k in range(PIECES):
                slot = row_slot(o, t, k)
                remote(
                    slot, slot, nz_sems.at[0, o, k], nz_sems.at[2, o, k], {"tp": mate}
                ).wait_recv()
                pass_rows(s, o, k)
                spread_rows(s, o, k)

    def hand_over(s, *origins):
        for o in origins:
            for k in range(PIECES):
                for dx in range(1, nx):
                    owner = lax.rem(x + nx - dx, nx) * 2 + c
                    arrived(row_slot(o, owner, k), nx_sems, o, dx, k)

                    def make(o=o, dx=dx, k=k):
                        slot = row_slot(o, lax.rem(x + nx - dx, nx) * 2 + c, k)
                        return remote(
                            slot, slot, nc_sems.at[0, o, dx, k], nc_sems.at[1, o, dx, k],
                            {"tp": mate},
                        )

                    launch(s, make)

    def rows_ready(o):
        for k in range(PIECES):
            for dx in range(nx):
                owner = lax.rem(x + nx - dx, nx) * 2 + 1 - c
                arrived(row_slot(o, owner, k), nc_sems, o, dx, k)

    def kv_in(s, o):
        for i in range(3):
            kv_arrived(o, i)
            if s < n - 1:
                kv_send(s, o, i)

    def kv_out(s):
        if s < n - 1:
            for i in range(3):
                kv_send(s, s, i)

    def prepare(s):
        for copy in own_copies(s):
            copy.start()
        size = size_of(s)
        if size < chunk:
            wg_all[:, size:] = jnp.zeros((n * depth, chunk - size), jnp.bfloat16)
            wu_all[:, size:] = jnp.zeros((n * depth, chunk - size), jnp.bfloat16)
            wd_all[size:, :] = jnp.zeros((chunk - size, n * dcols), jnp.bfloat16)
        for o in range(s, n - 1):
            k_all[o] = jnp.zeros_like(k_ref)
            v_all[o] = jnp.zeros_like(v_ref)
            gt_all[o] = jnp.zeros_like(gt_ref)

    def own_rows(s):
        for k in range(PIECES):
            pass_rows(s, s, k)
            spread_rows(s, s, k)

    steps = {
        "kv": kv_out,
        "kv_in": kv_in,
        "own": own_rows,
        "gu": lambda s, *to: weights(s, to, (GATE, UP)),
        "dn": lambda s, *to: weights(s, to, (DOWN,)),
        "in": lambda s, *origins: rows_in(s, *origins),
        "hand": lambda s, *origins: hand_over(s, *origins),
        "fwd": lambda s, e: relay_weights(s, e, (GATE, UP)),
        "fwd_dn": lambda s, e: relay_weights(s, e, (DOWN,)),
        "prep": prepare,
    }

    def follow(s, plan):
        for name, *where in plan:
            steps[name](s, *where)

    per_me(lambda s: follow(s, OPENING[s]))

    for copy in staged[3:]:
        copy.wait()
    pair = 128 // head
    lane = lax.broadcasted_iota(jnp.int32, (rows, 128), 1)
    causal = lax.broadcasted_iota(jnp.int32, (rows, rows), 0) >= lax.broadcasted_iota(
        jnp.int32, (rows, rows), 1
    )
    contract = (((1,), (1,)), ((), ()))
    filler = -heads % 8
    gates = gt_ref[...]
    if filler:
        gates = jnp.concatenate([gates, jnp.zeros((filler, rows), jnp.float32)], axis=0)
    gates = gates.T
    for p in range(heads // pair):
        cols = slice(p * 128, (p + 1) * 128)
        q_pair = q_ref[:, cols]
        joined = jnp.zeros((rows, 128), jnp.float32)
        for i in range(pair):
            h = p * pair + i
            inside = (lane >= i * head) & (lane < (i + 1) * head)
            q_head = jnp.where(inside, q_pair, jnp.zeros_like(q_pair))
            g_query = gates[:, h : h + 1]
            scores = []
            for o in range(n):
                k_pair = k_ref[:, cols] if o == n - 1 else k_all[o, :, cols]
                g_key = gt_ref[h : h + 1, :] if o == n - 1 else gt_all[o, h : h + 1, :]
                score = (
                    lax.dot_general(q_head, k_pair, contract, preferred_element_type=jnp.float32)
                    * head ** (-0.5)
                    + g_query
                    - g_key
                )
                allowed = causal if o == n - 1 else (jnp.zeros((rows, rows), jnp.int32) + me) > o
                scores.append(jnp.where(allowed, score, -1e30))
            peak = functools.reduce(
                jnp.maximum, [jnp.max(score, axis=-1, keepdims=True) for score in scores]
            )
            total = jnp.zeros((rows, 1), jnp.float32)
            summed = jnp.zeros((rows, 128), jnp.float32)
            for o in range(n):
                v_pair = v_ref[:, cols] if o == n - 1 else v_all[o, :, cols]
                weight = jnp.exp(scores[o] - peak)
                total += jnp.sum(weight, axis=-1, keepdims=True)
                summed += jnp.dot(
                    weight.astype(jnp.bfloat16), v_pair, preferred_element_type=jnp.float32
                )
            joined = jnp.where(inside, summed / total, joined)
        att[:, cols] = joined.astype(jnp.bfloat16)

    for k in range(width // 512):
        cols = slice(k * 512, (k + 1) * 512)
        proj[:, cols] = jnp.dot(
            att[...], w_out_ref[:, cols], preferred_element_type=jnp.float32
        ).astype(jnp.bfloat16)

    def block(index):
        return pl.ds(pl.multiple_of(index * sub, sub), sub)

    pc = [
        remote(
            proj.at[block(across(dx) * 2 + 1 - c)], pc_buf.at[dx],
            pc_sems.at[0, dx], pc_sems.at[1, dx], {"tp": mate},
        )
        for dx in range(nx)
    ]
    for dx in (*range(1, nx), 0):
        pc[dx].start()
    px = [
        remote(
            px_send.at[dx], px_buf.at[dx], px_sems.at[0, dx], px_sems.at[1, dx],
            {"tp": across(dx) * 2 + c},
        )
        for dx in range(nx)
    ]
    for dx in range(1, nx):
        pc[dx].wait_recv()
        px_send[dx] = (
            proj[block(across(dx) * 2 + c), :].astype(jnp.float32) + pc_buf[dx].astype(jnp.float32)
        ).astype(jnp.bfloat16)
        px[dx].start()
    pc[0].wait_recv()
    acc = proj[block(t), :].astype(jnp.float32) + pc_buf[0].astype(jnp.float32)
    for dx in range(1, nx):
        px[dx].wait_recv()
        acc += px_buf[dx].astype(jnp.float32)
    mix = (residual_ref[block(t), :].astype(jnp.float32) + acc).astype(jnp.bfloat16)
    mixed[...] = mix
    floats = mix.astype(jnp.float32)
    scale = lax.rsqrt(jnp.mean(floats * floats, axis=-1, keepdims=True) + 1e-06)
    normed[me, t] = (floats * scale * gain_ref[...]).astype(jnp.bfloat16)

    def exchange(s):
        follow(s, EXCHANGE[s])
        for e in range(n):
            if e != s:
                weights_there(s, e, (GATE, UP))
        for copy in own_copies(s):
            copy.wait()

    per_me(exchange)

    def span_of(e):
        return pl.ds(e * dcols if isinstance(e, int) else pl.multiple_of(e * dcols, 128), dcols)

    def c_copy(j, e):
        return remote(
            part.at[j, :, 1 - c, :, span_of(e)], c_buf.at[j, :, :, span_of(e)],
            c_sems.at[0, j, e], c_sems.at[1, j, e], {"tp": mate},
        )

    def x_copy(j, dx, e):
        return remote(
            x_send.at[j, dx, :, span_of(e)], x_buf.at[j, dx, :, span_of(e)],
            x_sems.at[0, j, dx, e], x_sems.at[1, j, dx, e], {"tp": across(dx) * 2 + c},
        )

    high = me // (n // 2)
    row_order = [me, me + 1 - 2 * lax.rem(me, 2), n // 2 - high, (n - 1) * (1 - high)]
    column_order = row_order

    def down_part(j, e):
        product = jnp.dot(
            hid[j], wd_all[:, span_of(e)], preferred_element_type=jnp.float32
        ).astype(jnp.bfloat16)
        part[j, :, :, :, span_of(e)] = product.reshape(nx, 2, sub, dcols)
        c_copy(j, e).start()

    def over_x(j, e):
        c_copy(j, e).wait_recv()
        for dx in range(1, nx):
            x_send[j, dx, :, span_of(e)] = (
                part[j, across(dx), c, :, span_of(e)].astype(jnp.float32)
                + c_buf[j, across(dx), :, span_of(e)].astype(jnp.float32)
            ).astype(jnp.bfloat16)
            x_copy(j, dx, e).start()

    def down_arrived(s, e):
        if (("fwd_dn", e)) not in EXCHANGE[s]:
            relay_weights(s, e, (DOWN,))

    def down_there(s, e):
        weights_there(s, e, (DOWN,))

    for k, j in enumerate(row_order):
        if k == 2:
            per_me(lambda s: follow(s, LATE[s]))
        per_me(lambda s: rows_ready(ROW_ORDER[s][k]))
        piece = normed[j].reshape(rows, width)
        gate = jnp.dot(piece, wg_all[...], preferred_element_type=jnp.float32)
        up = jnp.dot(piece, wu_all[...], preferred_element_type=jnp.float32)
        hid[j] = (gate / (1.0 + jnp.exp(-gate)) * up).astype(jnp.bfloat16)
        down_part(j, column_order[0])
        if k:
            over_x(row_order[k - 1], column_order[0])
    per_me(lambda s: down_arrived(s, COLUMN_ORDER[s][2]))
    over_x(row_order[-1], column_order[0])

    def local_sum(j, e):
        acc = part[j, x, c, :, span_of(e)].astype(jnp.float32) + c_buf[
            j, x, :, span_of(e)
        ].astype(jnp.float32)
        for dx in range(1, nx):
            x_copy(j, dx, e).wait_recv()
            acc += x_buf[j, dx, :, span_of(e)].astype(jnp.float32)
        return acc

    def z_in(slot, e):
        place = z_buf.at[slot, :, span_of(e)]
        remote(
            place, place, z_sems.at[0, slot, e], z_sems.at[1, slot, e], {"tp": mate}
        ).wait_recv()
        return z_buf[slot, :, span_of(e)].astype(jnp.float32)

    def over_z(s, j, e):
        acc = local_sum(j, e)
        if direct(n, j > s, e):
            to, slot = j, n + 1 + s
        else:
            to = s + 1 if j > s else s - 1
            slot = n if to == j and j < s else j
            if 0 <= (s - 1 if j > s else s + 1) < n:
                acc += z_in(j, e)
        z_send[j, :, span_of(e)] = acc.astype(jnp.bfloat16)

        def make():
            return remote(
                z_send.at[j, :, span_of(e)], z_buf.at[slot, :, span_of(e)],
                z_sems.at[0, j, e], z_sems.at[1, slot, e], {"sp": to},
            )

        launch(s, make)

    def finish(s, e):
        acc = local_sum(s, e)
        for up, others, slot in ((True, range(s), s), (False, range(s + 1, n), n)):
            if direct(n, up, e):
                for b in others:
                    acc += z_in(n + 1 + b, e)
            elif others:
                acc += z_in(slot, e)
        total_ref[:, span_of(e)] = mixed[:, span_of(e)].astype(jnp.float32) + 0.5 * acc

    order = line_tasks(n)

    def along(s, due):
        for j, e in order[s]:
            if stage(n, s, j, e) == due:
                if j == s:
                    finish(s, e)
                else:
                    over_z(s, j, e)

    for q in range(1, n):
        if q == 1:
            per_me(lambda s: down_arrived(s, COLUMN_ORDER[s][1]))
        per_me(lambda s: down_there(s, COLUMN_ORDER[s][q]))
        for j in row_order[::-1]:
            down_part(j, column_order[q])
        for j in row_order[::-1]:
            over_x(j, column_order[q])
        if q == 1:
            per_me(lambda s: down_arrived(s, COLUMN_ORDER[s][3]))
        if q < 3:
            per_me(lambda s: along(s, q - 1))

    per_me(lambda s: along(s, 2))
    summed = total_ref[...]
    scale = lax.rsqrt(jnp.mean(summed * summed, axis=-1, keepdims=True) + 1e-06)
    out_ref[...] = (summed * scale).astype(jnp.bfloat16)

    for copy in pc:
        copy.wait_send()
    for dx in range(1, nx):
        px[dx].wait_send()
    for e in range(n):
        for j in range(n):
            c_copy(j, e).wait_send()
            for dx in range(1, nx):
                x_copy(j, dx, e).wait_send()

    def all_sent(s):
        for make in sent[s]:
            make().wait_send()

    per_me(all_sent)


def fused_body(residual, queries, keys, values, log_gates, w_out, norm_gain, w_gate, w_up, w_down):
    n, tp = lax.axis_size("sp"), lax.axis_size("tp")
    rows, width = residual.shape
    sub = rows // tp
    nx = tp // 2
    depth, ff = w_gate.shape
    dcols = w_down.shape[1]
    chunk = window(ff, n)
    gates_t = log_gates.T
    bf16, f32 = jnp.bfloat16, jnp.float32
    shapes = [
        (queries.shape, bf16),
        (keys.shape, bf16),
        (values.shape, bf16),
        (gates_t.shape, f32),
        (residual.shape, bf16),
        (w_out.shape, bf16),
        ((1, width), f32),
        ((n - 1, *keys.shape), bf16),
        ((n - 1, *values.shape), bf16),
        ((n - 1, *gates_t.shape), f32),
        (queries.shape, bf16),
        ((rows, width), bf16),
        ((nx, sub, width), bf16),
        ((nx, sub, width), bf16),
        ((nx, sub, width), bf16),
        ((sub, width), bf16),
        ((n, tp, sub, width), bf16),
        ((n * depth, chunk), bf16),
        ((n * depth, chunk), bf16),
        ((chunk, n * dcols), bf16),
        ((n, rows, chunk), bf16),
        ((n, nx, 2, sub, width), bf16),
        ((n, nx, sub, width), bf16),
        ((n, nx, sub, width), bf16),
        ((n, nx, sub, width), bf16),
        ((n, sub, width), bf16),
        ((2 * n + 1, sub, width), bf16),
        ((sub, width), f32),
    ]
    sems = [
        (2, n, 3),
        (2, n, 3),
        (2, n, 3),
        (2, nx),
        (2, nx),
        (3, n, PIECES),
        (2, n, nx, PIECES),
        (2, n, nx, PIECES),
        (2, n, n),
        (2, n, nx, n),
        (2, 2 * n + 1, n),
        (3,),
        (7,),
    ]
    return pl.pallas_call(
        functools.partial(layer_kernel, n, tp, chunk),
        out_shape=jax.ShapeDtypeStruct((sub, width), bf16),
        in_specs=[pl.BlockSpec(memory_space=pl.ANY)] * 10,
        out_specs=pl.BlockSpec(memory_space=pltpu.VMEM),
        scratch_shapes=[pltpu.VMEM(shape, dtype) for shape, dtype in shapes]
        + [pltpu.SemaphoreType.DMA(shape) for shape in sems],
        compiler_params=pltpu.CompilerParams(
            collective_id=0, has_side_effects=True, vmem_limit_bytes=60 * 1024 * 1024
        ),
    )(
        queries, keys, values, gates_t, residual, w_out, norm_gain[None, :],
        w_gate, w_up, w_down,
    )


def window(ff, n):
    return -(-ff // (n * 128)) * 128


def fits(mesh, shapes):
    residual, queries, gates, gate = shapes
    n, tp, grp = mesh.shape["sp"], mesh.shape["tp"], mesh.shape["grp"]
    ff = gate[1] // tp
    heads = gates[1] // tp
    head = queries[1] // gates[1]
    rows = residual[0] // (grp * n)
    return (
        grp == 2
        and n == 4
        and tp % 2 == 0
        and ff % 128 == 0
        and window(ff, n) * (n - 1) < ff
        and 128 % head == 0
        and (heads * head) % 128 == 0
        and rows % (16 * tp) == 0
        and rows * n * residual[1] <= 1 << 21
    )


def solution(mesh):
    in_specs = (
        P(("grp", "sp"), None),
        P(("grp", "sp"), "tp"),
        P(("grp", "sp"), "tp"),
        P(("grp", "sp"), "tp"),
        P(("grp", "sp"), "tp"),
        P("tp", None),
        P(),
        P("sp", "tp"),
        P("sp", "tp"),
        P("tp", "sp"),
    )
    out_specs = P(("grp", "sp", "tp"), None)

    def layer(*args):
        residual, queries, _, _, log_gates, _, _, w_gate, _, _ = args
        shapes = (residual.shape, queries.shape, log_gates.shape, w_gate.shape)
        chosen = fused_body if fits(mesh, shapes) else body
        return jax.shard_map(
            chosen, mesh=mesh, in_specs=in_specs, out_specs=out_specs, check_vma=False
        )(*args)

    return layer
```

```python
import functools
import math

import jax
import jax.numpy as jnp
from jax import lax
from jax.experimental import pallas as pl
from jax.experimental.pallas import tpu as pltpu
from jax.sharding import PartitionSpec as P


def normalize(rows_in, gain):
    floats = rows_in.astype(jnp.float32)
    scaled = floats * lax.rsqrt(jnp.mean(floats * floats, axis=-1, keepdims=True) + 1e-06)
    return (scaled * gain).astype(jnp.bfloat16)


def attend(queries, keys, values, log_gates):
    row_count = queries.shape[0]
    head_count = log_gates.shape[1]
    head_width = queries.shape[1] // head_count
    score_scale = head_width ** (-0.5)
    first_row = lax.axis_index("sp") * row_count
    query_heads = queries.reshape(row_count, head_count, head_width)
    query_gates = log_gates.T
    query_positions = first_row + jnp.arange(row_count, dtype=jnp.int32)
    initial = (
        jnp.full((head_count, row_count), -1e30, jnp.float32),
        jnp.zeros((head_count, row_count), jnp.float32),
        jnp.zeros((head_count, row_count, head_width), jnp.float32),
    )
    carried = initial
    key_piece = lax.all_gather(keys.astype(jnp.float32), "sp", axis=0, tiled=True).astype(
        jnp.bfloat16
    )
    value_piece = lax.all_gather(values.astype(jnp.float32), "sp", axis=0, tiled=True).astype(
        jnp.bfloat16
    )
    gate_piece = lax.all_gather(log_gates, "sp", axis=0, tiled=True)
    length = key_piece.shape[0]
    block_rows = math.gcd(length, 2048)
    block_count = length // block_rows
    key_blocks = key_piece.reshape(block_count, block_rows, head_count, head_width)
    value_blocks = value_piece.reshape(block_count, block_rows, head_count, head_width)
    gate_blocks = gate_piece.reshape(block_count, block_rows, head_count)
    offsets = jnp.arange(block_count, dtype=jnp.int32) * block_rows

    def one_block(state, inputs):
        current_key_block, value_block, gate_block, offset = inputs

        def work(current):
            running_max, running_sum, accumulated = current
            scores = (
                jnp.einsum(
                    "qhd,khd->hqk",
                    query_heads,
                    current_key_block,
                    preferred_element_type=jnp.float32,
                )
                * score_scale
            )
            scores = scores + query_gates[:, :, None] - gate_block.T[:, None, :]
            key_positions = offset + jnp.arange(block_rows, dtype=jnp.int32)
            causal = (query_positions[:, None] >= key_positions[None, :])[None]
            scores = jnp.where(causal, scores, -1e30)
            new_max = jnp.maximum(running_max, jnp.max(scores, axis=-1))
            weights = jnp.where(causal, jnp.exp(scores - new_max[:, :, None]), 0.0)
            rescale = jnp.exp(running_max - new_max)
            running_sum = running_sum * rescale + jnp.sum(weights, axis=-1)
            product = jnp.einsum(
                "hqk,khd->hqd",
                weights.astype(jnp.bfloat16),
                value_block,
                preferred_element_type=jnp.float32,
            )
            accumulated = accumulated * rescale[:, :, None] + product
            return (new_max, running_sum, accumulated)

        state = lax.cond(offset <= first_row + row_count - 1, work, lambda current: current, state)
        return (state, None)

    carried, _ = lax.scan(one_block, carried, (key_blocks, value_blocks, gate_blocks, offsets))
    running_max, running_sum, accumulated = carried
    attended = accumulated / running_sum[:, :, None]
    return (
        attended.transpose(1, 0, 2).reshape(row_count, head_count * head_width).astype(jnp.bfloat16)
    )


def body(residual, queries, keys, values, log_gates, w_out, norm_gain, w_gate, w_up, w_down):
    attended = attend(queries, keys, values, log_gates)
    row_count = attended.shape[0]
    per_device = row_count // lax.axis_size("tp")
    my_first = lax.axis_index("tp") * per_device
    projected = lax.psum(
        jnp.dot(attended, w_out, preferred_element_type=jnp.float32).astype(jnp.bfloat16), "tp"
    ).astype(jnp.float32)
    mixed_all = (residual.astype(jnp.float32) + projected).astype(jnp.bfloat16)
    normed_all = normalize(mixed_all, norm_gain)
    mixed = lax.dynamic_slice_in_dim(mixed_all, my_first, per_device, 0)
    gate_whole = lax.all_gather(w_gate, "sp", axis=0, tiled=True)
    up_whole = lax.all_gather(w_up, "sp", axis=0, tiled=True)
    down_whole = lax.all_gather(w_down, "sp", axis=1, tiled=True)
    gate_proj = jnp.dot(normed_all, gate_whole, preferred_element_type=jnp.float32)
    up_proj = jnp.dot(normed_all, up_whole, preferred_element_type=jnp.float32)
    hidden = (jax.nn.silu(gate_proj) * up_proj).astype(jnp.bfloat16)
    down_sum = lax.psum_scatter(
        jnp.dot(hidden, down_whole, preferred_element_type=jnp.float32).astype(jnp.bfloat16),
        "tp",
        scatter_dimension=0,
        tiled=True,
    ).astype(jnp.float32)
    summed = mixed.astype(jnp.float32) + 0.5 * down_sum
    scaled = summed * lax.rsqrt(jnp.mean(summed * summed, axis=-1, keepdims=True) + 1e-06)
    return scaled.astype(jnp.bfloat16)


MESH = pl.DeviceIdType.MESH
PIECES = 2
OPENING = (
    (("kv",), ("gu", 1), ("dn", 1), ("gu", 2, 3), ("prep",)),
    (("kv",), ("gu", 0), ("dn", 0), ("prep",), ("kv_in", 0), ("gu", 2, 3), ("fwd", 2)),
    (("kv",), ("gu", 1, 0), ("prep",), ("kv_in", 1), ("kv_in", 0), ("gu", 3), ("dn", 3), ("fwd", 3)),
    (("gu", 2), ("dn", 2), ("gu", 1, 0), ("prep",), ("kv_in", 2), ("kv_in", 1), ("kv_in", 0)),
)
EXCHANGE = (
    (
        ("own",), ("fwd", 1), ("hand", 0), ("fwd", 3), ("fwd", 2), ("fwd_dn", 1), ("in", 1),
        ("in", 2), ("hand", 1), ("in", 3), ("dn", 2, 3), ("hand", 2),
    ),
    (
        ("own",), ("fwd", 0), ("fwd", 3), ("hand", 1), ("fwd_dn", 0), ("in", 2), ("in", 0),
        ("dn", 2, 3), ("in", 3), ("hand", 2), ("hand", 0),
    ),
    (
        ("own",), ("fwd", 0), ("hand", 2), ("in", 3), ("dn", 1, 0), ("fwd_dn", 3), ("fwd", 1),
        ("in", 1), ("hand", 3), ("in", 0), ("hand", 1),
    ),
    (
        ("own",), ("fwd", 2), ("fwd", 0), ("hand", 3), ("fwd_dn", 2), ("in", 2), ("fwd", 1),
        ("in", 1), ("dn", 1, 0), ("hand", 2), ("in", 0), ("hand", 1),
    ),
)
LATE = ((("hand", 3),), (("hand", 3),), (("hand", 0),), (("hand", 0),))
STARTS = (2.0, 9.5, 15.5, 19.5)


def direct(n, up, e):
    return e == (n - 1 if up else 0)


def stage(n, s, j, e):
    lower = s < n // 2
    if j == s or (j > s) != lower or (e < n // 2) != lower:
        return 2
    if s in (0, n - 1):
        return 0 if e == s else 1
    return 1 if e in (0, n - 1) else 2


ROW_ORDER = ((0, 1, 2, 3), (1, 0, 2, 3), (2, 3, 1, 0), (3, 2, 1, 0))
COLUMN_ORDER = ((0, 1, 2, 3), (1, 0, 2, 3), (2, 3, 1, 0), (3, 2, 1, 0))


def line_tasks(n):
    wire, hop, add = 1.4, 3.5, 0.3
    base = (STARTS[1] + 2, STARTS[2] + 1, STARTS[3] + 1)
    term, clock = {}, [0.0] * n
    for s in range(n):
        link = 0.0
        for q, e in enumerate(COLUMN_ORDER[s]):
            for p in range(n):
                j = ROW_ORDER[s][p if q == 0 else n - 1 - p]
                link = max(link, STARTS[q] + (1.6 if q == 0 else 0.2) * p) + wire
                term[s, j, e] = link + hop
    waiting = {(s, j, e) for s in range(n) for j in range(n) for e in range(n) if j != s}
    arrival, links, tasks = {}, {}, [[] for _ in range(n)]
    while waiting:
        best = None
        for s, j, e in waiting:
            up = j > s
            behind = s - 1 if up else s + 1
            if 0 <= behind < n and (s, j, e) not in arrival and not direct(n, up, e):
                continue
            start = max(term[s, j, e], clock[s], base[stage(n, s, j, e)])
            start = max(start, arrival.get((s, j, e), 0.0))
            best = min(best or (start + 1, 0, 0), (start, -abs(j - s), (s, j, e)))
        start, _, (s, j, e) = best
        waiting.remove((s, j, e))
        tasks[s].append((j, e))
        up = j > s
        clock[s] = start + add
        links[s, up] = max(links.get((s, up), 0.0), start + add) + wire
        if not direct(n, up, e):
            arrival[s + 1 if up else s - 1, j, e] = links[s, up] + hop
    for s in range(n):
        tasks[s] += [(s, e) for e in COLUMN_ORDER[s]]
    return tasks


def layer_kernel(
    n, tp, chunk,
    q_in, k_in, v_in, gt_in, residual_in, w_out_in, gain_in, wg_ref, wu_ref, wd_ref,
    out_ref,
    q_ref, k_ref, v_ref, gt_ref, residual_ref, w_out_ref, gain_ref,
    k_all, v_all, gt_all, att, proj, pc_buf, px_send, px_buf, mixed, normed,
    wg_all, wu_all, wd_all, hid, part, c_buf, x_send, x_buf, z_send, z_buf, total_ref,
    kv_sems, w_sems, y_sems, pc_sems, px_sems, nz_sems, nx_sems, nc_sems, c_sems, x_sems, z_sems, o_sems, i_sems,
):
    me = lax.axis_index("sp")
    t = lax.axis_index("tp")
    g = lax.axis_index("grp")
    x, c = t // 2, t % 2
    nx = tp // 2
    mate = x * 2 + (1 - c)
    rows = q_ref.shape[0]
    sub = rows // tp
    width = residual_ref.shape[1]
    heads = gt_ref.shape[0]
    head = q_ref.shape[1] // heads
    depth = wg_ref.shape[0]
    ff = wg_ref.shape[1]
    half = depth // 2
    dcols = wd_ref.shape[1]
    dhalf = dcols // 2
    GATE, UP, DOWN = range(3)

    def across(dx):
        return lax.rem(x + dx, nx)

    def per_me(work):
        for s in range(n):

            @pl.when(me == s)
            def _(s=s):
                work(s)

    def remote(src, dst, send_sem, recv_sem, target):
        return pltpu.make_async_remote_copy(
            src_ref=src, dst_ref=dst, send_sem=send_sem, recv_sem=recv_sem,
            device_id=target, device_id_type=MESH,
        )

    def arrived(slot, sems, *index):
        remote(slot, slot, sems.at[(0, *index)], sems.at[(1, *index)], {"tp": mate}).wait_recv()

    barrier = pltpu.get_barrier_semaphore()
    for d in range(1, n):
        pl.semaphore_signal(barrier, inc=1, device_id={"sp": lax.rem(me + d, n)}, device_id_type=MESH)
    for dx in range(1, nx):
        pl.semaphore_signal(
            barrier, inc=1, device_id={"tp": across(dx) * 2 + c}, device_id_type=MESH
        )
    pl.semaphore_signal(barrier, inc=1, device_id={"tp": mate}, device_id_type=MESH)
    pl.semaphore_signal(barrier, inc=1, device_id={"grp": 1 - g}, device_id_type=MESH)
    staged = [
        pltpu.make_async_copy(src, dst, i_sems.at[i])
        for i, (src, dst) in enumerate(
            (
                (k_in, k_ref), (v_in, v_ref), (gt_in, gt_ref), (q_in, q_ref),
                (w_out_in, w_out_ref), (residual_in, residual_ref), (gain_in, gain_ref),
            )
        )
    ]
    for copy in staged:
        copy.start()
    for copy in staged[:3]:
        copy.wait()
    pl.semaphore_wait(barrier, n - 1 + nx - 1 + 2)

    sent = [[] for _ in range(n)]

    def launch(s, make):
        make().start()
        sent[s].append(make)

    def kv_copy(s, o, i):
        own = (k_ref, v_ref, gt_ref)[i]
        held = (k_all, v_all, gt_all)[i].at[min(o, n - 2)]
        return remote(
            own if o == s else held, held, kv_sems.at[0, o, i], kv_sems.at[1, o, i], {"sp": s + 1}
        )

    def kv_send(s, o, i):
        launch(s, lambda: kv_copy(s, o, i))

    def kv_arrived(o, i):
        arrived((k_all, v_all, gt_all)[i].at[o], kv_sems, o, i)

    def size_of(j):
        return min(chunk, ff - j * chunk)

    def weight_slot(s, e, i, side):
        size = size_of(s)
        if i == DOWN:
            return wd_all.at[
                :size, pl.ds(pl.multiple_of(e * dcols + side * dhalf, 128), dhalf)
            ]
        held = (wg_all, wu_all)[i]
        return held.at[pl.ds(pl.multiple_of(e * depth + side * half, 16), half), :size]

    def weight_copy(s, j, i):
        place = pl.ds(j * chunk, size_of(j))
        if i == DOWN:
            src = wd_ref.at[place, pl.ds(pl.multiple_of(g * dhalf, 128), dhalf)]
        else:
            src = (wg_ref, wu_ref)[i].at[pl.ds(pl.multiple_of(g * half, 16), half), place]
        return remote(
            src, weight_slot(j, s, i, g), w_sems.at[0, j, i], w_sems.at[1, s, i], {"sp": j}
        )

    def weights(s, targets, pieces):
        for j in targets:
            for i in pieces:
                launch(s, lambda j=j, i=i: weight_copy(s, j, i))

    def relay_weights(s, e, pieces):
        for i in pieces:
            slot = weight_slot(s, e, i, g)
            arrived(slot, w_sems, e, i)

            def make(i=i):
                place = weight_slot(s, e, i, g)
                return remote(
                    place, place, y_sems.at[0, e, i], y_sems.at[1, e, i], {"grp": 1 - g}
                )

            launch(s, make)

    def weights_there(s, e, pieces):
        for i in pieces:
            arrived(weight_slot(s, e, i, 1 - g), y_sems, e, i)

    def own_copies(s):
        size = size_of(s)
        mine = pl.ds(s * chunk, size)
        return (
            pltpu.make_async_copy(
                wg_ref.at[:, mine], wg_all.at[pl.ds(s * depth, depth), :size], o_sems.at[0]
            ),
            pltpu.make_async_copy(
                wu_ref.at[:, mine], wu_all.at[pl.ds(s * depth, depth), :size], o_sems.at[1]
            ),
            pltpu.make_async_copy(
                wd_ref.at[mine, :], wd_all.at[:size, pl.ds(s * dcols, dcols)], o_sems.at[2]
            ),
        )

    span = width // PIECES

    def row_slot(o, owner, k):
        return normed.at[o, owner, :, k * span : (k + 1) * span]

    def pass_rows(s, o, k):
        for way, j in ((0, s + 1), (1, s - 1)):
            if 0 <= j < n and (o == s or (o < s) == (way == 0)):

                def make(way=way, j=j):
                    slot = row_slot(o, t, k)
                    return remote(
                        slot, slot, nz_sems.at[way, o, k], nz_sems.at[2, o, k], {"sp": j}
                    )

                launch(s, make)

    def spread_rows(s, o, k):
        def to_mate():
            slot = row_slot(o, t, k)
            return remote(slot, slot, nc_sems.at[0, o, 0, k], nc_sems.at[1, o, 0, k], {"tp": mate})

        for dx in range(1, nx):

            def over(dx=dx):
                slot = row_slot(o, t, k)
                return remote(
                    slot, slot, nx_sems.at[0, o, dx, k], nx_sems.at[1, o, dx, k],
                    {"tp": across(dx) * 2 + c},
                )

            launch(s, over)
        launch(s, to_mate)

    def rows_in(s, *origins):
        for o in origins:
            for k in range(PIECES):
                slot = row_slot(o, t, k)
                remote(
                    slot, slot, nz_sems.at[0, o, k], nz_sems.at[2, o, k], {"tp": mate}
                ).wait_recv()
                pass_rows(s, o, k)
                spread_rows(s, o, k)

    def hand_over(s, *origins):
        for o in origins:
            for k in range(PIECES):
                for dx in range(1, nx):
                    owner = lax.rem(x + nx - dx, nx) * 2 + c
                    arrived(row_slot(o, owner, k), nx_sems, o, dx, k)

                    def make(o=o, dx=dx, k=k):
                        slot = row_slot(o, lax.rem(x + nx - dx, nx) * 2 + c, k)
                        return remote(
                            slot, slot, nc_sems.at[0, o, dx, k], nc_sems.at[1, o, dx, k],
                            {"tp": mate},
                        )

                    launch(s, make)

    def rows_ready(o):
        for k in range(PIECES):
            for dx in range(nx):
                owner = lax.rem(x + nx - dx, nx) * 2 + 1 - c
                arrived(row_slot(o, owner, k), nc_sems, o, dx, k)

    def kv_in(s, o):
        for i in range(3):
            kv_arrived(o, i)
            if s < n - 1:
                kv_send(s, o, i)

    def kv_out(s):
        if s < n - 1:
            for i in range(3):
                kv_send(s, s, i)

    def prepare(s):
        for copy in own_copies(s):
            copy.start()
        size = size_of(s)
        if size < chunk:
            wg_all[:, size:] = jnp.zeros((n * depth, chunk - size), jnp.bfloat16)
            wu_all[:, size:] = jnp.zeros((n * depth, chunk - size), jnp.bfloat16)
            wd_all[size:, :] = jnp.zeros((chunk - size, n * dcols), jnp.bfloat16)
        for o in range(s, n - 1):
            k_all[o] = jnp.zeros_like(k_ref)
            v_all[o] = jnp.zeros_like(v_ref)
            gt_all[o] = jnp.zeros_like(gt_ref)

    def own_rows(s):
        for k in range(PIECES):
            pass_rows(s, s, k)
            spread_rows(s, s, k)

    steps = {
        "kv": kv_out,
        "kv_in": kv_in,
        "own": own_rows,
        "gu": lambda s, *to: weights(s, to, (GATE, UP)),
        "dn": lambda s, *to: weights(s, to, (DOWN,)),
        "in": lambda s, *origins: rows_in(s, *origins),
        "hand": lambda s, *origins: hand_over(s, *origins),
        "fwd": lambda s, e: relay_weights(s, e, (GATE, UP)),
        "fwd_dn": lambda s, e: relay_weights(s, e, (DOWN,)),
        "prep": prepare,
    }

    def follow(s, plan):
        for name, *where in plan:
            steps[name](s, *where)

    per_me(lambda s: follow(s, OPENING[s]))

    for copy in staged[3:]:
        copy.wait()
    pair = 128 // head
    lane = lax.broadcasted_iota(jnp.int32, (rows, 128), 1)
    causal = lax.broadcasted_iota(jnp.int32, (rows, rows), 0) >= lax.broadcasted_iota(
        jnp.int32, (rows, rows), 1
    )
    contract = (((1,), (1,)), ((), ()))
    filler = -heads % 8
    gates = gt_ref[...]
    if filler:
        gates = jnp.concatenate([gates, jnp.zeros((filler, rows), jnp.float32)], axis=0)
    gates = gates.T
    for p in range(heads // pair):
        cols = slice(p * 128, (p + 1) * 128)
        q_pair = q_ref[:, cols]
        joined = jnp.zeros((rows, 128), jnp.float32)
        for i in range(pair):
            h = p * pair + i
            inside = (lane >= i * head) & (lane < (i + 1) * head)
            q_head = jnp.where(inside, q_pair, jnp.zeros_like(q_pair))
            g_query = gates[:, h : h + 1]
            scores = []
            for o in range(n):
                k_pair = k_ref[:, cols] if o == n - 1 else k_all[o, :, cols]
                g_key = gt_ref[h : h + 1, :] if o == n - 1 else gt_all[o, h : h + 1, :]
                score = (
                    lax.dot_general(q_head, k_pair, contract, preferred_element_type=jnp.float32)
                    * head ** (-0.5)
                    + g_query
                    - g_key
                )
                allowed = causal if o == n - 1 else (jnp.zeros((rows, rows), jnp.int32) + me) > o
                scores.append(jnp.where(allowed, score, -1e30))
            peak = functools.reduce(
                jnp.maximum, [jnp.max(score, axis=-1, keepdims=True) for score in scores]
            )
            total = jnp.zeros((rows, 1), jnp.float32)
            summed = jnp.zeros((rows, 128), jnp.float32)
            for o in range(n):
                v_pair = v_ref[:, cols] if o == n - 1 else v_all[o, :, cols]
                weight = jnp.exp(scores[o] - peak)
                total += jnp.sum(weight, axis=-1, keepdims=True)
                summed += jnp.dot(
                    weight.astype(jnp.bfloat16), v_pair, preferred_element_type=jnp.float32
                )
            joined = jnp.where(inside, summed / total, joined)
        att[:, cols] = joined.astype(jnp.bfloat16)

    for k in range(width // 512):
        cols = slice(k * 512, (k + 1) * 512)
        proj[:, cols] = jnp.dot(
            att[...], w_out_ref[:, cols], preferred_element_type=jnp.float32
        ).astype(jnp.bfloat16)

    def block(index):
        return pl.ds(pl.multiple_of(index * sub, sub), sub)

    pc = [
        remote(
            proj.at[block(across(dx) * 2 + 1 - c)], pc_buf.at[dx],
            pc_sems.at[0, dx], pc_sems.at[1, dx], {"tp": mate},
        )
        for dx in range(nx)
    ]
    for dx in (*range(1, nx), 0):
        pc[dx].start()
    px = [
        remote(
            px_send.at[dx], px_buf.at[dx], px_sems.at[0, dx], px_sems.at[1, dx],
            {"tp": across(dx) * 2 + c},
        )
        for dx in range(nx)
    ]
    for dx in range(1, nx):
        pc[dx].wait_recv()
        px_send[dx] = (
            proj[block(across(dx) * 2 + c), :].astype(jnp.float32) + pc_buf[dx].astype(jnp.float32)
        ).astype(jnp.bfloat16)
        px[dx].start()
    pc[0].wait_recv()
    acc = proj[block(t), :].astype(jnp.float32) + pc_buf[0].astype(jnp.float32)
    for dx in range(1, nx):
        px[dx].wait_recv()
        acc += px_buf[dx].astype(jnp.float32)
    mix = (residual_ref[block(t), :].astype(jnp.float32) + acc).astype(jnp.bfloat16)
    mixed[...] = mix
    floats = mix.astype(jnp.float32)
    scale = lax.rsqrt(jnp.mean(floats * floats, axis=-1, keepdims=True) + 1e-06)
    normed[me, t] = (floats * scale * gain_ref[...]).astype(jnp.bfloat16)

    def exchange(s):
        follow(s, EXCHANGE[s])
        for e in range(n):
            if e != s:
                weights_there(s, e, (GATE, UP))
        for copy in own_copies(s):
            copy.wait()

    per_me(exchange)

    def span_of(e):
        return pl.ds(e * dcols if isinstance(e, int) else pl.multiple_of(e * dcols, 128), dcols)

    def c_copy(j, e):
        return remote(
            part.at[j, :, 1 - c, :, span_of(e)], c_buf.at[j, :, :, span_of(e)],
            c_sems.at[0, j, e], c_sems.at[1, j, e], {"tp": mate},
        )

    def x_copy(j, dx, e):
        return remote(
            x_send.at[j, dx, :, span_of(e)], x_buf.at[j, dx, :, span_of(e)],
            x_sems.at[0, j, dx, e], x_sems.at[1, j, dx, e], {"tp": across(dx) * 2 + c},
        )

    high = me // (n // 2)
    row_order = [me, me + 1 - 2 * lax.rem(me, 2), n // 2 - high, (n - 1) * (1 - high)]
    column_order = row_order

    def down_part(j, e):
        product = jnp.dot(
            hid[j], wd_all[:, span_of(e)], preferred_element_type=jnp.float32
        ).astype(jnp.bfloat16)
        part[j, :, :, :, span_of(e)] = product.reshape(nx, 2, sub, dcols)
        c_copy(j, e).start()

    def over_x(j, e):
        c_copy(j, e).wait_recv()
        for dx in range(1, nx):
            x_send[j, dx, :, span_of(e)] = (
                part[j, across(dx), c, :, span_of(e)].astype(jnp.float32)
                + c_buf[j, across(dx), :, span_of(e)].astype(jnp.float32)
            ).astype(jnp.bfloat16)
            x_copy(j, dx, e).start()

    def down_arrived(s, e):
        if (("fwd_dn", e)) not in EXCHANGE[s]:
            relay_weights(s, e, (DOWN,))

    def down_there(s, e):
        weights_there(s, e, (DOWN,))

    for k, j in enumerate(row_order):
        if k == 2:
            per_me(lambda s: follow(s, LATE[s]))
        per_me(lambda s: rows_ready(ROW_ORDER[s][k]))
        piece = normed[j].reshape(rows, width)
        gate = jnp.dot(piece, wg_all[...], preferred_element_type=jnp.float32)
        up = jnp.dot(piece, wu_all[...], preferred_element_type=jnp.float32)
        hid[j] = (gate / (1.0 + jnp.exp(-gate)) * up).astype(jnp.bfloat16)
        down_part(j, column_order[0])
        if k:
            over_x(row_order[k - 1], column_order[0])
    per_me(lambda s: down_arrived(s, COLUMN_ORDER[s][2]))
    over_x(row_order[-1], column_order[0])

    def local_sum(j, e):
        acc = part[j, x, c, :, span_of(e)].astype(jnp.float32) + c_buf[
            j, x, :, span_of(e)
        ].astype(jnp.float32)
        for dx in range(1, nx):
            x_copy(j, dx, e).wait_recv()
            acc += x_buf[j, dx, :, span_of(e)].astype(jnp.float32)
        return acc

    def z_in(slot, e):
        place = z_buf.at[slot, :, span_of(e)]
        remote(
            place, place, z_sems.at[0, slot, e], z_sems.at[1, slot, e], {"tp": mate}
        ).wait_recv()
        return z_buf[slot, :, span_of(e)].astype(jnp.float32)

    def over_z(s, j, e):
        acc = local_sum(j, e)
        if direct(n, j > s, e):
            to, slot = j, n + 1 + s
        else:
            to = s + 1 if j > s else s - 1
            slot = n if to == j and j < s else j
            if 0 <= (s - 1 if j > s else s + 1) < n:
                acc += z_in(j, e)
        z_send[j, :, span_of(e)] = acc.astype(jnp.bfloat16)

        def make():
            return remote(
                z_send.at[j, :, span_of(e)], z_buf.at[slot, :, span_of(e)],
                z_sems.at[0, j, e], z_sems.at[1, slot, e], {"sp": to},
            )

        launch(s, make)

    def finish(s, e):
        acc = local_sum(s, e)
        for up, others, slot in ((True, range(s), s), (False, range(s + 1, n), n)):
            if direct(n, up, e):
                for b in others:
                    acc += z_in(n + 1 + b, e)
            elif others:
                acc += z_in(slot, e)
        total_ref[:, span_of(e)] = mixed[:, span_of(e)].astype(jnp.float32) + 0.5 * acc

    order = line_tasks(n)

    def along(s, due):
        for j, e in order[s]:
            if stage(n, s, j, e) == due:
                if j == s:
                    finish(s, e)
                else:
                    over_z(s, j, e)

    for q in range(1, n):
        if q == 1:
            per_me(lambda s: down_arrived(s, COLUMN_ORDER[s][1]))
        per_me(lambda s: down_there(s, COLUMN_ORDER[s][q]))
        for j in row_order[::-1]:
            down_part(j, column_order[q])
        for j in row_order[::-1]:
            over_x(j, column_order[q])
        if q == 1:
            per_me(lambda s: down_arrived(s, COLUMN_ORDER[s][3]))
        if q < 3:
            per_me(lambda s: along(s, q - 1))

    per_me(lambda s: along(s, 2))
    summed = total_ref[...]
    scale = lax.rsqrt(jnp.mean(summed * summed, axis=-1, keepdims=True) + 1e-06)
    out_ref[...] = (summed * scale).astype(jnp.bfloat16)

    for copy in pc:
        copy.wait_send()
    for dx in range(1, nx):
        px[dx].wait_send()
    for e in range(n):
        for j in range(n):
            c_copy(j, e).wait_send()
            for dx in range(1, nx):
                x_copy(j, dx, e).wait_send()

    def all_sent(s):
        for make in sent[s]:
            make().wait_send()

    per_me(all_sent)


def fused_body(residual, queries, keys, values, log_gates, w_out, norm_gain, w_gate, w_up, w_down):
    n, tp = lax.axis_size("sp"), lax.axis_size("tp")
    rows, width = residual.shape
    sub = rows // tp
    nx = tp // 2
    depth, ff = w_gate.shape
    dcols = w_down.shape[1]
    chunk = window(ff, n)
    gates_t = log_gates.T
    bf16, f32 = jnp.bfloat16, jnp.float32
    shapes = [
        (queries.shape, bf16),
        (keys.shape, bf16),
        (values.shape, bf16),
        (gates_t.shape, f32),
        (residual.shape, bf16),
        (w_out.shape, bf16),
        ((1, width), f32),
        ((n - 1, *keys.shape), bf16),
        ((n - 1, *values.shape), bf16),
        ((n - 1, *gates_t.shape), f32),
        (queries.shape, bf16),
        ((rows, width), bf16),
        ((nx, sub, width), bf16),
        ((nx, sub, width), bf16),
        ((nx, sub, width), bf16),
        ((sub, width), bf16),
        ((n, tp, sub, width), bf16),
        ((n * depth, chunk), bf16),
        ((n * depth, chunk), bf16),
        ((chunk, n * dcols), bf16),
        ((n, rows, chunk), bf16),
        ((n, nx, 2, sub, width), bf16),
        ((n, nx, sub, width), bf16),
        ((n, nx, sub, width), bf16),
        ((n, nx, sub, width), bf16),
        ((n, sub, width), bf16),
        ((2 * n + 1, sub, width), bf16),
        ((sub, width), f32),
    ]
    sems = [
        (2, n, 3),
        (2, n, 3),
        (2, n, 3),
        (2, nx),
        (2, nx),
        (3, n, PIECES),
        (2, n, nx, PIECES),
        (2, n, nx, PIECES),
        (2, n, n),
        (2, n, nx, n),
        (2, 2 * n + 1, n),
        (3,),
        (7,),
    ]
    return pl.pallas_call(
        functools.partial(layer_kernel, n, tp, chunk),
        out_shape=jax.ShapeDtypeStruct((sub, width), bf16),
        in_specs=[pl.BlockSpec(memory_space=pl.ANY)] * 10,
        out_specs=pl.BlockSpec(memory_space=pltpu.VMEM),
        scratch_shapes=[pltpu.VMEM(shape, dtype) for shape, dtype in shapes]
        + [pltpu.SemaphoreType.DMA(shape) for shape in sems],
        compiler_params=pltpu.CompilerParams(
            collective_id=0, has_side_effects=True, vmem_limit_bytes=60 * 1024 * 1024
        ),
    )(
        queries, keys, values, gates_t, residual, w_out, norm_gain[None, :],
        w_gate, w_up, w_down,
    )


def window(ff, n):
    return -(-ff // (n * 128)) * 128


def fits(mesh, shapes):
    residual, queries, gates, gate = shapes
    n, tp, grp = mesh.shape["sp"], mesh.shape["tp"], mesh.shape["grp"]
    ff = gate[1] // tp
    heads = gates[1] // tp
    head = queries[1] // gates[1]
    rows = residual[0] // (grp * n)
    return (
        grp == 2
        and n == 4
        and tp % 2 == 0
        and ff % 128 == 0
        and window(ff, n) * (n - 1) < ff
        and 128 % head == 0
        and (heads * head) % 128 == 0
        and rows % (16 * tp) == 0
        and rows * n * residual[1] <= 1 << 21
    )


def solution(mesh):
    in_specs = (
        P(("grp", "sp"), None),
        P(("grp", "sp"), "tp"),
        P(("grp", "sp"), "tp"),
        P(("grp", "sp"), "tp"),
        P(("grp", "sp"), "tp"),
        P("tp", None),
        P(),
        P("sp", "tp"),
        P("sp", "tp"),
        P("tp", "sp"),
    )
    out_specs = P(("grp", "sp", "tp"), None)

    def layer(*args):
        residual, queries, _, _, log_gates, _, _, w_gate, _, _ = args
        shapes = (residual.shape, queries.shape, log_gates.shape, w_gate.shape)
        chosen = fused_body if fits(mesh, shapes) else body
        return jax.shard_map(
            chosen, mesh=mesh, in_specs=in_specs, out_specs=out_specs, check_vma=False
        )(*args)

    return layer
```
